32 devices in a mesh: dp: 4 (over y, x), kv: 4 (over z), tp: 2 (over core).
Axes of the slice: x: 2, y: 2, z: 4, core: 2. Of those that a mesh axis runs over, the one named last changes fastest.
Arguments:
- tokens: bfloat16 [8192, 2048], P(('dp', 'kv')), parts along dimension 0, may hold values from -60 to 60, as said below
- chosen: int32 [128, 16], P(('dp', 'kv')), parts along dimension 0, may hold values from -1 to 31, as said below
- query_weight: bfloat16 [2048, 1024], P('kv', 'tp'), may hold values from -0.125 to 0.125
- key_matrix: bfloat16 [2048, 128], P('kv', 'tp'), may hold values from -0.125 to 0.125
- value_matrix: bfloat16 [2048, 128], P('kv', 'tp'), may hold values from -0.125 to 0.125
- out_weight: bfloat16 [1024, 2048], P('tp', 'kv'), may hold values from -0.1875 to 0.1875
- out_gain: float32 [2048], replicated, may hold values from 0.1 to 1.9
Outputs:
- mixed_out: bfloat16 [8192, 2048], P(('dp', 'kv', 'tp')), parts along dimension 0
The draws below stay inside these ranges and needn't reach their ends.
There are 4 independent parts, one for each index of `dp`. The reference program is written for one: setup_inputs(seed, part) draws one part's arguments, and reference() takes and returns one part's arrays. A program takes and returns all parts, laid end to end along the dimension named above; an argument that names none is the same for every part. Nothing has to cross between parts.
Inputs may be any that keep to these rules, and one draw needn't show every extreme that they name: tokens are of order one apart from few rows. chosen[g, 0] = g; every other entry of row g is -1 or a block below g, and the entries of a row other than -1 are distinct; the blocks that the rows of one device name on any single other device are at most 2 different ones, and this is reached.
All inputs are finite; a program needn't handle non-finite values.
Results may differ from the reference program's by a relative error of at most 0.012.
The reference program's roundings to bfloat16 on the way count: a program that leaves them out, or rounds other values in their place, can miss the bound.
Values may be sent and summed in bfloat16 or wider, within the bound.
A program may use at most 64 MiB of HBM per device.

```python
import jax
import jax.numpy as jnp
from jax import lax

MODEL_WIDTH = 2048
QUERY_HEADS = 16
KEY_VALUE_HEADS = 2
HEAD_WIDTH = 64
BLOCK_LENGTH = 64
SEL = 16
CAP = 2
SEQ = 2048
BLOCKS_DEV = 8
SEQUENCE_BLOCKS = 32
N_KV = 4


def draw_tokens(key, part):
    base = jax.random.normal(key, (SEQ, MODEL_WIDTH), jnp.float32)
    return jnp.clip(base, -60.0, 60.0).astype(jnp.bfloat16)


def draw_chosen(key, part):
    owners = N_KV
    per_dev = BLOCKS_DEV
    parts_keys = jax.random.split(key, 3)
    requester = jnp.arange(owners, dtype=jnp.int32)[:, None]
    holder = jnp.arange(owners, dtype=jnp.int32)[None, :]
    roll = jax.random.randint(parts_keys[0], (owners, owners), 0, 8)
    favored = (holder == 0) | (holder == requester - 1) | (holder == requester - owners // 2)
    counts = jnp.where(favored | (roll < 2), CAP, jnp.where(roll < 4, 1, 0))
    counts = jnp.where(holder < requester, counts, 0)
    order = jax.random.randint(parts_keys[1], (owners, owners, per_dev), 0, 1 << 20) * 1024 + jnp.arange(per_dev, dtype=jnp.int32)
    _, first = lax.top_k(order, min(CAP, per_dev))
    first = jnp.concatenate([first, jnp.zeros((owners, owners, CAP - first.shape[-1]), jnp.int32)], axis=-1)
    slot_index = jnp.arange(CAP, dtype=jnp.int32)
    counts = jnp.minimum(counts, per_dev)
    remote_ids = (holder[:, :, None] * per_dev + first).reshape(owners, owners * CAP)
    remote_live = (slot_index[None, None, :] < counts[:, :, None]).reshape(owners, owners * CAP)
    remote_tier = jnp.broadcast_to(jnp.where(favored, 2, 1)[:, :, None], (owners, owners, CAP)).reshape(owners, owners * CAP)
    local_pos = jnp.arange(per_dev, dtype=jnp.int32)
    local_ids = jnp.broadcast_to((requester * per_dev + local_pos[None, :])[:, None, :], (owners, per_dev, per_dev))
    local_live = jnp.broadcast_to((local_pos[None, :] < local_pos[:, None])[None], (owners, per_dev, per_dev))
    pad_ids = jnp.zeros((owners, per_dev, SEL), jnp.int32)
    pad_live = jnp.zeros((owners, per_dev, SEL), bool)
    cand_ids = jnp.concatenate([jnp.broadcast_to(remote_ids[:, None, :], (owners, per_dev, owners * CAP)), local_ids, pad_ids], axis=-1)
    cand_live = jnp.concatenate([jnp.broadcast_to(remote_live[:, None, :], (owners, per_dev, owners * CAP)), local_live, pad_live], axis=-1)
    cand_tier = jnp.concatenate([jnp.broadcast_to(remote_tier[:, None, :], (owners, per_dev, owners * CAP)), jnp.ones((owners, per_dev, per_dev), jnp.int32), jnp.zeros((owners, per_dev, SEL), jnp.int32)], axis=-1)
    cand_width = owners * CAP + per_dev + SEL
    cand_index = jnp.arange(cand_width, dtype=jnp.int32)[None, None, :]
    noise = jax.random.randint(parts_keys[2], (owners, per_dev, cand_width), 0, 1 << 17)
    score = jnp.where(cand_live, cand_tier * (1 << 28) + noise * 2048 + cand_index, cand_index)
    _, position = lax.top_k(score, SEL - 1)
    taken = jnp.take_along_axis(cand_ids, position, axis=-1)
    live = jnp.take_along_axis(cand_live, position, axis=-1)
    others = jnp.where(live, taken, -1)
    own_ids = (requester * per_dev + local_pos[None, :])[:, :, None]
    return jnp.concatenate([own_ids, others], axis=-1).reshape(owners * per_dev, SEL).astype(jnp.int32)


def block_scale(key, dims, cuts, smallest, high):
    def one(dim, parts):
        heights = jax.random.uniform(jax.random.fold_in(jax.random.fold_in(key, 6), dim), (parts,), jnp.float32, smallest / len(cuts), high / len(cuts))
        return jnp.repeat(jnp.exp(heights), dims[dim] // parts).reshape((-1,) + (1,) * (len(dims) - dim - 1))

    gain = one(*cuts[0])
    for cut in cuts[1:]:
        gain = gain * one(*cut)
    return gain


def centred(stream_key, shape, spread, reach, shards=(), kind=jnp.bfloat16):
    gain = block_scale(stream_key, shape, shards, -0.22, 0.18) if shards else 1.0
    array = jax.random.normal(stream_key, shape, jnp.float32) * spread * gain
    return jnp.minimum(jnp.maximum(array, -reach), reach).astype(kind)


def setup_inputs(seed: int = 0, part: int = 0) -> dict:
    splits = jax.random.split(jax.random.key(seed), 8)
    own_keys = jax.random.split(jax.random.fold_in(splits[7], part), 8)
    return {
        "tokens": draw_tokens(jax.random.fold_in(jax.random.fold_in(splits[7], part), 71), part),
        "chosen": draw_chosen(jax.random.fold_in(jax.random.fold_in(splits[7], part), 71), part),
        "query_weight": centred(splits[2], (MODEL_WIDTH, QUERY_HEADS * HEAD_WIDTH), MODEL_WIDTH ** -0.5, 0.125, ((0, 4), (1, 2))),
        "key_matrix": centred(splits[3], (MODEL_WIDTH, KEY_VALUE_HEADS * HEAD_WIDTH), MODEL_WIDTH ** -0.5, 0.125, ((0, 4), (1, 2))),
        "value_matrix": centred(splits[4], (MODEL_WIDTH, KEY_VALUE_HEADS * HEAD_WIDTH), MODEL_WIDTH ** -0.5, 0.125, ((0, 4), (1, 2))),
        "out_weight": centred(splits[5], (QUERY_HEADS * HEAD_WIDTH, MODEL_WIDTH), (QUERY_HEADS * HEAD_WIDTH) ** -0.5, 0.1875, ((0, 2), (1, 4))),
        "out_gain": jnp.clip(1.0 + 0.18 * jax.random.normal(splits[6], (MODEL_WIDTH,), jnp.float32), 0.1, 1.9),
    }


def reference(tokens, chosen, query_weight, key_matrix, value_matrix, out_weight, out_gain):
    head_groups = QUERY_HEADS // KEY_VALUE_HEADS
    query_rows = jnp.dot(tokens, query_weight, preferred_element_type=jnp.float32).astype(jnp.bfloat16)
    key_rows = jnp.dot(tokens, key_matrix, preferred_element_type=jnp.float32).astype(jnp.bfloat16)
    value_rows = jnp.dot(tokens, value_matrix, preferred_element_type=jnp.float32).astype(jnp.bfloat16)
    blocked_queries = query_rows.reshape(SEQUENCE_BLOCKS, BLOCK_LENGTH, KEY_VALUE_HEADS, head_groups, HEAD_WIDTH)
    blocked_keys = key_rows.reshape(SEQUENCE_BLOCKS, BLOCK_LENGTH, KEY_VALUE_HEADS, HEAD_WIDTH)
    blocked_values = value_rows.reshape(SEQUENCE_BLOCKS, BLOCK_LENGTH, KEY_VALUE_HEADS, HEAD_WIDTH)
    offsets = jnp.arange(BLOCK_LENGTH, dtype=jnp.int32)
    score_scale = HEAD_WIDTH ** (-0.5)

    def one_block(inputs):
        block, row_ids, index = inputs
        safe_ids = jnp.maximum(row_ids, 0).astype(jnp.int32)
        picked_keys = blocked_keys[safe_ids].astype(jnp.float32)
        picked_values = blocked_values[safe_ids].astype(jnp.float32)
        query_pos = index * BLOCK_LENGTH + offsets
        key_pos = safe_ids[:, None] * BLOCK_LENGTH + offsets[None, :]
        visible = (row_ids >= 0)[None, :, None] & (key_pos[None, :, :] <= query_pos[:, None, None])
        scores = jnp.einsum('qhgd,skhd->hgqsk', block.astype(jnp.float32), picked_keys) * score_scale
        scores = jnp.where(visible[None, None], scores, -1e+30)
        row_max = lax.optimization_barrier(jnp.max(scores, axis=(3, 4), keepdims=True))
        expon = jnp.exp(scores - row_max)
        row_sum = lax.optimization_barrier(jnp.sum(expon, axis=(3, 4), keepdims=True))
        weights_bf = (expon / row_sum).astype(jnp.bfloat16)
        result = jnp.einsum('hgqsk,skhd->qhgd', weights_bf.astype(jnp.float32), picked_values)
        return result.astype(jnp.bfloat16)
    attended = lax.map(one_block, (blocked_queries, chosen, jnp.arange(SEQUENCE_BLOCKS, dtype=jnp.int32)))
    attended = attended.reshape(SEQ, QUERY_HEADS * HEAD_WIDTH)
    mixed = jnp.dot(attended, out_weight, preferred_element_type=jnp.float32)
    normed = mixed * lax.rsqrt(lax.optimization_barrier(jnp.mean(mixed * mixed, axis=-1, keepdims=True)) + 1e-06) * out_gain.astype(jnp.float32)
    return normed.astype(jnp.bfloat16)
```

```python
import functools

import jax
import jax.numpy as jnp
from jax import lax
from jax.experimental import pallas as pl
from jax.experimental.pallas import tpu as pltpu
from jax.sharding import PartitionSpec as P

HEAD_WIDTH = 64
BLOCK_LENGTH = 64
LANES = 2 * HEAD_WIDTH
HIDDEN = -1e30
CAP = 2
PIECES = (1, 2, 2)


def remote(src, dst, send, recv, axis, peer):
    return pltpu.make_async_remote_copy(
        src_ref=src,
        dst_ref=dst,
        send_sem=send,
        recv_sem=recv,
        device_id={axis: peer},
        device_id_type=pl.DeviceIdType.MESH,
    )


def fused(
    n_dp, n_kv, n_tp,
    chosen_hbm, tokens_hbm, key_hbm, value_hbm, query_hbm, out_hbm, gain_hbm, result,
    chosen, gain, tokens, pair_own, query_own, out_own, wanted, asks, packed, kv_own, kv_far,
    pair_all, query_all, out_all, kv_all, vk_all, query_sum, query_rows, attended,
    leaving, arriving, kept,
    load_sem, z_send, z_recv, f_send, d_send, d_recv, r_send, r_recv, kv_send, kv_recv, t_send, t_recv, ask_send, ask_recv,
):
    d, z, t = lax.axis_index("dp"), lax.axis_index("kv"), lax.axis_index("tp")
    rows, width = tokens.shape
    blocks = rows // BLOCK_LENGTH
    depth = width // n_kv
    half = rows // n_tp
    cut = depth // n_dp
    loads = [
        pltpu.make_async_copy(source, target, load_sem.at[k])
        for k, (source, target) in enumerate(
            ((query_hbm, query_own), (tokens_hbm, tokens), (out_hbm, out_own),
             (gain_hbm, gain), (chosen_hbm, wanted), (chosen_hbm, chosen))
        )
    ]
    pair_loads = [
        pltpu.make_async_copy(
            source.at[:, k * cut : (k + 1) * cut],
            pair_own.at[k, side * HEAD_WIDTH : (side + 1) * HEAD_WIDTH],
            load_sem.at[6 + k * 2 + side],
        )
        for k in range(n_dp)
        for side, source in enumerate((key_hbm, value_hbm))
    ]
    for load in pair_loads + loads:
        load.start()

    barrier = pltpu.get_barrier_semaphore()
    for axis, me, count in (("dp", d, n_dp), ("kv", z, n_kv), ("tp", t, n_tp)):
        for step in range(1, count):
            pl.semaphore_signal(
                barrier, inc=1, device_id={axis: lax.rem(me + step, count)},
                device_id_type=pl.DeviceIdType.MESH,
            )
    pl.semaphore_wait(barrier, n_dp + n_kv + n_tp - 3)

    owns = (pair_own, query_own, out_own)
    alls = (pair_all, query_all, out_all)
    events = [
        (which, part, j) for which in range(3) for part in range(PIECES[which]) for j in range(1, n_kv)
    ]
    origin = (z, z + 1 - 2 * lax.rem(z, 2), lax.rem(z + 2, 4), 3 - z)
    middle = (z == 1) | (z == 2)
    near = (d, d + 1 - 2 * lax.rem(d, 2), lax.rem(d + 2, 4))
    corner = 3 - d

    def span_of(e, share=0, shares=1):
        which, part, _ = events[e]
        size = owns[which].shape[1] // PIECES[which]
        return pl.ds(part * size + share * (size // shares), size // shares)

    def first(e):
        which, _, j = events[e]
        return remote(
            owns[which].at[d, span_of(e)], alls[which].at[z, d, span_of(e)],
            z_send.at[e], z_recv.at[e], "kv", origin[j],
        )

    def first_in(e):
        which, _, j = events[e]
        slot = alls[which].at[origin[j], d, span_of(e)]
        return remote(slot, slot, z_send.at[e], z_recv.at[e], "kv", origin[j])

    def onward(e):
        which, _, j = events[e]
        slot = alls[which].at[origin[j], d, span_of(e)]
        return remote(slot, slot, f_send.at[e], z_recv.at[e + 1], "kv", origin[1])

    def second(e, k, place=None):
        which, _, j = events[e]
        slot = alls[which].at[origin[j], d if place is None else place, span_of(e)]
        return remote(slot, slot, d_send.at[e, k], d_recv.at[e, k], "dp", near[k])

    def halfway(e, k, place):
        which, _, j = events[e]
        slot = alls[which].at[origin[j], place, span_of(e, k - 1, 2)]
        return remote(slot, slot, r_send.at[e, k], r_recv.at[e, k], "dp", near[3 - k])

    def out(e):
        if events[e][2] == 3:

            @pl.when(middle)
            def _():
                first(e).start()
        else:
            first(e).start()

    def pass_on(e):
        first_in(e).wait_recv()
        if events[e][2] == 2:

            @pl.when(middle)
            def _():
                onward(e).start()

        for k in (1, 2):
            second(e, k).start()

    def relay(e):
        for k in (1, 2):
            second(e, k, near[k]).wait_recv()
            halfway(e, k, near[k]).start()

    def take(e):
        for k in (1, 2):
            halfway(e, k, corner).wait_recv()

    def whole(which, j):
        block = owns[which][...] if j == 0 else alls[which][origin[j]]
        return block.reshape(block.shape[0] * block.shape[1], block.shape[2])

    def token_part(j):
        start = pl.multiple_of(origin[j] * depth, depth)
        return tokens[:, pl.ds(start, depth)]

    def ask(j):
        return remote(wanted, asks.at[z], ask_send.at[j], ask_recv.at[j], "kv", origin[j])

    def ask_in(j):
        slot = asks.at[origin[j]]
        return remote(slot, slot, ask_send.at[j], ask_recv.at[j], "kv", origin[j])

    loads[4].wait()
    for j in range(1, n_kv):
        ask(j).start()
    for load in pair_loads:
        load.wait()
    for e in (1, 0):
        out(e)
    loads[0].wait()
    for e in (3, 4):
        out(e)
    pass_on(0)
    out(2)
    pass_on(1)
    out(7)
    pass_on(3)
    for e in (6, 5, 8):
        out(e)
    loads[2].wait()
    out(13)
    relay(0)
    pass_on(2)
    relay(1)
    pass_on(4)
    out(10)
    relay(3)
    out(9)
    take(0)
    relay(2)
    for e in (7, 6):
        pass_on(e)
    take(1)
    out(12)
    take(2)
    pass_on(5)
    for load in loads[1:2] + loads[3:4] + loads[5:]:
        load.wait()

    def pair_part(j):
        block = pair_own[...] if j == 0 else pair_all[origin[j]]
        block = jnp.concatenate([block[k] for k in range(n_dp)], axis=1)
        return lax.dot_general(
            token_part(j), block, (((1,), (1,)), ((), ())), preferred_element_type=jnp.float32
        )

    total = pair_part(0)
    for j in range(1, n_kv):
        total += pair_part(j)
    kv_own[...] = total.astype(jnp.bfloat16).reshape(blocks, BLOCK_LENGTH, LANES)

    def named(rows_of, owner):
        local = rows_of - owner * blocks
        inside = (local >= 0) & (local < blocks)
        return (
            jnp.min(jnp.where(inside, local, blocks - 1)),
            jnp.max(jnp.where(inside, local, 0)),
        )

    def kv_out(j):
        return remote(
            packed.at[j], kv_far.at[pl.ds(z * CAP, CAP)], kv_send.at[j], kv_recv.at[j],
            "kv", origin[j],
        )

    def kv_in(j):
        slot = kv_far.at[pl.ds(origin[j] * CAP, CAP)]
        return remote(slot, slot, kv_send.at[j], kv_recv.at[j], "kv", origin[j])

    kv_far[pl.ds(z * CAP, CAP)] = jnp.zeros((CAP, BLOCK_LENGTH, LANES), jnp.bfloat16)
    for j in range(1, n_kv):
        ask_in(j).wait_recv()
        lowest, highest = named(asks[origin[j]], z)
        packed[j, 0] = kv_own[lowest]
        packed[j, 1] = kv_own[highest]
    firsts = [named(wanted[...], owner)[0] + owner * blocks for owner in range(n_kv)]
    pass_on(8)
    for e in (7, 6):
        relay(e)
    for j in range(1, n_kv):
        kv_out(j).start()
    relay(4)
    take(3)
    relay(5)
    query_sum[...] = jnp.dot(token_part(0), whole(1, 0), preferred_element_type=jnp.float32)
    relay(8)
    take(7)
    for e in (13, 9, 12):
        pass_on(e)
    out(14)
    take(6)
    out(11)
    take(4)
    query_sum[...] += jnp.dot(
        token_part(1), whole(1, 1), preferred_element_type=jnp.float32
    )
    pass_on(10)
    take(5)
    query_sum[...] += jnp.dot(
        token_part(2), whole(1, 2), preferred_element_type=jnp.float32
    )
    take(8)
    query_sum[...] += jnp.dot(
        token_part(3), whole(1, 3), preferred_element_type=jnp.float32
    )
    query_rows[...] = query_sum[...].astype(jnp.bfloat16) * jnp.bfloat16(HEAD_WIDTH ** (-0.5))
    for j in range(1, n_kv):
        kv_in(j).wait_recv()

    swap = (
        lax.rem(lax.broadcasted_iota(jnp.int32, (LANES, LANES), 0) + HEAD_WIDTH, LANES)
        == lax.broadcasted_iota(jnp.int32, (LANES, LANES), 1)
    ).astype(jnp.float32).astype(jnp.bfloat16)
    for source, start in ((kv_far, 0), (kv_own, n_kv * CAP)):
        count = source.shape[0]
        part = source[...]
        turned = jnp.dot(
            part.reshape(count * BLOCK_LENGTH, LANES), swap, preferred_element_type=jnp.float32
        )
        kv_all[start : start + count] = part
        vk_all[start : start + count] = turned.astype(jnp.bfloat16).reshape(part.shape)

    pass_on(14)

    picks = chosen.shape[1]
    pairs = query_rows.shape[1] // LANES

    def attend(b, carry):
        @pl.when(b == 2)
        def _():
            pass_on(11)
            relay(9)

        @pl.when(b == 4)
        def _():
            for e in (12, 13):
                relay(e)

        @pl.when(b == 5)
        def _():
            for e in (14, 10):
                relay(e)

        @pl.when(b == 6)
        def _():
            relay(11)

        lane = lax.broadcasted_iota(jnp.int32, (BLOCK_LENGTH, LANES), 1)
        row = lax.broadcasted_iota(jnp.int32, (BLOCK_LENGTH, LANES), 0)
        low = (lane < HEAD_WIDTH).astype(jnp.float32)
        names = [chosen[b, s] for s in range(picks)]
        offs = [jnp.where(name >= 0, 0.0, HIDDEN) for name in names]
        bias = []
        for s in range(0, picks, 2):
            tile = jnp.where(lane < HEAD_WIDTH, offs[s], offs[s + 1])
            if s == 0:
                tile = jnp.where((lane < HEAD_WIDTH) & (lane > row), HIDDEN, tile)
            bias.append(tile)
        bias = jnp.concatenate(bias, axis=1)

        def place(name):
            name = jnp.maximum(name, 0)
            spot = name - z * blocks + n_kv * CAP
            for owner in range(n_kv):
                local = name - owner * blocks
                away = (local >= 0) & (local < blocks) & (z != owner)
                far = owner * CAP + jnp.where(name == firsts[owner], 0, 1)
                spot = jnp.where(away, far, spot)
            return spot

        safe = [jnp.where(name >= 0, place(name), 0) for name in names]
        kv = jnp.concatenate([kv_all[g] for g in safe], axis=0)
        vk = jnp.concatenate([vk_all[g] for g in safe], axis=0)
        at = pl.ds(pl.multiple_of(b * BLOCK_LENGTH, BLOCK_LENGTH), BLOCK_LENGTH)
        query = query_rows[at, :]
        stacked = jnp.concatenate(
            [query[:, p * LANES : (p + 1) * LANES] for p in range(pairs)], axis=0
        )
        keep = jnp.concatenate([low] * pairs, axis=0)
        outs = []
        for side in range(2):
            mask = keep if side == 0 else 1.0 - keep
            masked = stacked * mask.astype(jnp.bfloat16)
            keys, values = (kv, vk) if side == 0 else (vk, kv)
            scores = lax.dot_general(
                masked, keys, (((1,), (1,)), ((), ())), preferred_element_type=jnp.float32
            )
            scores = scores.reshape(pairs, BLOCK_LENGTH, picks * BLOCK_LENGTH) + bias[None]
            top = jnp.max(scores, axis=2, keepdims=True)
            expon = jnp.exp(scores - top)
            inverse = 1.0 / jnp.sum(expon, axis=2, keepdims=True)
            probs = expon.astype(jnp.bfloat16)
            probs = probs.reshape(pairs * BLOCK_LENGTH, picks * BLOCK_LENGTH)
            out = jnp.dot(probs, values, preferred_element_type=jnp.float32)
            outs.append(out * inverse.reshape(pairs * BLOCK_LENGTH, 1))
        joined = jnp.where(keep > 0.5, outs[0], outs[1]).astype(jnp.bfloat16)
        for p in range(pairs):
            attended[at, p * LANES : (p + 1) * LANES] = joined[
                p * BLOCK_LENGTH : (p + 1) * BLOCK_LENGTH
            ]
        return carry

    lax.fori_loop(0, blocks, attend, 0)

    peer = lax.rem(t + 1, n_tp)
    other_rows = attended[pl.ds(pl.multiple_of(peer * half, half), half), :]
    own_rows = attended[pl.ds(pl.multiple_of(t * half, half), half), :]

    def swap_half(j):
        return remote(
            leaving.at[origin[j]], arriving.at[origin[j]], t_send.at[j], t_recv.at[j], "tp", peer
        )

    def project(j):
        weight = whole(2, j)
        leaving[origin[j]] = jnp.dot(
            other_rows, weight, preferred_element_type=jnp.float32
        ).astype(jnp.bfloat16)
        swap_half(j).start()
        kept[origin[j]] = jnp.dot(own_rows, weight, preferred_element_type=jnp.float32)

    for e in (13, 9):
        take(e)
    project(0)
    take(12)
    project(1)
    take(10)
    project(2)
    for e in (11, 14):
        take(e)
    project(3)

    square = jnp.zeros((half, 1), jnp.float32)
    for j in range(n_kv):
        slot = origin[j]
        swap_half(j).wait_recv()
        mixed = kept[slot] + arriving[slot].astype(jnp.float32)
        kept[slot] = mixed
        square += jnp.sum(mixed * mixed, axis=1, keepdims=True)
    scale = lax.rsqrt(square * (1.0 / width) + 1e-06)
    for j in range(n_kv):
        columns = slice(j * depth, (j + 1) * depth)
        result[:, columns] = (kept[j] * scale * gain[:, columns]).astype(jnp.bfloat16)

    for e in range(len(events)):
        if events[e][2] < 3:
            first(e).wait_send()
        for k in (1, 2):
            second(e, k).wait_send()
            halfway(e, k, near[k]).wait_send()

    @pl.when(middle)
    def _():
        for e in range(len(events)):
            if events[e][2] == 3:
                first(e).wait_send()
            if events[e][2] == 2:
                onward(e).wait_send()

    for j in range(1, n_kv):
        kv_out(j).wait_send()
        ask(j).wait_send()
    for j in range(n_kv):
        swap_half(j).wait_send()


def per_device_fused(
    n_dp, n_kv, n_tp,
    tokens, chosen, query_weight, key_matrix, value_matrix, out_weight, out_gain,
):
    rows, width = tokens.shape
    depth, columns = query_weight.shape
    blocks = rows // BLOCK_LENGTH
    cut = lambda w: w.reshape(n_dp, w.shape[0] // n_dp, w.shape[1])
    query, out = cut(query_weight), cut(out_weight)
    pair = jax.ShapeDtypeStruct((n_dp, LANES, depth // n_dp), jnp.bfloat16)
    bf16, f32 = jnp.bfloat16, jnp.float32
    vmem = pl.BlockSpec(memory_space=pltpu.VMEM)
    off_core = pl.BlockSpec(memory_space=pltpu.HBM)
    dma = pltpu.SemaphoreType.DMA
    copies = sum(PIECES) * (n_kv - 1)
    return pl.pallas_call(
        functools.partial(fused, n_dp, n_kv, n_tp),
        out_shape=pltpu.VMEM((rows // n_tp, width), bf16),
        in_specs=[
            off_core, off_core, off_core, off_core, off_core, off_core, off_core,
        ],
        out_specs=vmem,
        scratch_shapes=[
            pltpu.SMEM((blocks, chosen.shape[1]), jnp.int32),
            pltpu.VMEM((1, width), f32),
            pltpu.VMEM((rows, width), bf16),
            pltpu.VMEM(pair.shape, bf16),
            pltpu.VMEM(query.shape, bf16),
            pltpu.VMEM(out.shape, bf16),
            pltpu.VMEM((blocks, chosen.shape[1]), jnp.int32),
            pltpu.VMEM((n_kv, blocks, chosen.shape[1]), jnp.int32),
            pltpu.VMEM((n_kv, CAP, BLOCK_LENGTH, LANES), bf16),
            pltpu.VMEM((blocks, BLOCK_LENGTH, LANES), bf16),
            pltpu.VMEM((n_kv * CAP, BLOCK_LENGTH, LANES), bf16),
            pltpu.VMEM((n_kv,) + pair.shape, bf16),
            pltpu.VMEM((n_kv,) + query.shape, bf16),
            pltpu.VMEM((n_kv,) + out.shape, bf16),
            pltpu.VMEM((n_kv * CAP + blocks, BLOCK_LENGTH, LANES), bf16),
            pltpu.VMEM((n_kv * CAP + blocks, BLOCK_LENGTH, LANES), bf16),
            pltpu.VMEM((rows, columns), f32),
            pltpu.VMEM((rows, columns), bf16),
            pltpu.VMEM((rows, columns), bf16),
            pltpu.VMEM((n_kv, rows // n_tp, width // n_kv), bf16),
            pltpu.VMEM((n_kv, rows // n_tp, width // n_kv), bf16),
            pltpu.VMEM((n_kv, rows // n_tp, width // n_kv), f32),
            dma((6 + 2 * n_dp,)), dma((copies,)), dma((copies,)), dma((copies,)),
            dma((copies, 3)), dma((copies, 3)), dma((copies, 3)), dma((copies, 3)),
            dma((n_kv,)), dma((n_kv,)), dma((n_kv,)), dma((n_kv,)),
            dma((n_kv,)), dma((n_kv,)),
        ],
        compiler_params=pltpu.CompilerParams(
            collective_id=0, has_side_effects=True, vmem_limit_bytes=54 * 1024 * 1024
        ),
    )(chosen, tokens, key_matrix.T, value_matrix.T, query, out, out_gain.reshape(1, width))


def per_device(tokens, chosen, query_weight, key_matrix, value_matrix, out_weight, out_gain):
    tok_rows = tokens.shape[0]
    blocks = tok_rows // BLOCK_LENGTH
    device = lax.axis_index("kv")
    kv_count = lax.axis_size("kv")
    whole_query, whole_key, whole_value = (
        lax.all_gather(query_weight, "kv", axis=0, tiled=True),
        lax.all_gather(key_matrix, "kv", axis=0, tiled=True),
        lax.all_gather(value_matrix, "kv", axis=0, tiled=True),
    )
    query_rows = jnp.dot(tokens, whole_query, preferred_element_type=jnp.float32).astype(
        jnp.bfloat16
    )
    key_rows = jnp.dot(tokens, whole_key, preferred_element_type=jnp.float32).astype(jnp.bfloat16)
    value_rows = jnp.dot(tokens, whole_value, preferred_element_type=jnp.float32).astype(
        jnp.bfloat16
    )
    paired = jnp.concatenate([key_rows, value_rows], axis=1)
    pair_width = paired.shape[1]
    safe_ids = jnp.maximum(chosen, 0)
    everyone = lax.all_gather(paired, "kv", axis=0, tiled=True).reshape(
        kv_count * blocks, BLOCK_LENGTH, pair_width
    )
    picked = jnp.take(everyone, safe_ids, axis=0)
    head_count = query_rows.shape[1] // HEAD_WIDTH
    grouped = query_rows.reshape(blocks, BLOCK_LENGTH, head_count, HEAD_WIDTH)
    offsets = jnp.arange(BLOCK_LENGTH, dtype=jnp.int32)
    query_pos = (device * blocks + jnp.arange(blocks, dtype=jnp.int32))[
        :, None
    ] * BLOCK_LENGTH + offsets[None, :]
    key_pos = safe_ids[:, :, None] * BLOCK_LENGTH + offsets[None, None, :]
    visible = (chosen >= 0)[:, None, :, None] & (
        key_pos[:, None, :, :] <= query_pos[:, :, None, None]
    )

    def attend_block(inputs):
        query_block, pair_block, seen = inputs
        block_keys = pair_block[..., :HEAD_WIDTH]
        block_values = pair_block[..., HEAD_WIDTH:]
        scores = jnp.einsum(
            "qgd,skd->gqsk", query_block, block_keys, preferred_element_type=jnp.float32
        ) * HEAD_WIDTH ** (-0.5)
        scores = jnp.where(seen[None], scores, -1e30)
        row_max = jnp.max(scores, axis=(2, 3), keepdims=True)
        expon = jnp.exp(scores - row_max)
        row_sum = jnp.sum(expon, axis=(2, 3), keepdims=True)
        weights_bf = (expon / row_sum).astype(jnp.bfloat16)
        result = jnp.einsum(
            "gqsk,skd->qgd", weights_bf, block_values, preferred_element_type=jnp.float32
        )
        return result.astype(jnp.bfloat16)

    attended = lax.map(attend_block, (grouped, picked, visible))
    attended = attended.reshape(tok_rows, head_count * HEAD_WIDTH)
    whole_out = lax.all_gather(out_weight, "kv", axis=1, tiled=True)
    mixed = lax.psum_scatter(
        jnp.dot(attended, whole_out, preferred_element_type=jnp.float32).astype(jnp.bfloat16),
        "tp",
        scatter_dimension=0,
        tiled=True,
    ).astype(jnp.float32)
    normed = mixed * lax.rsqrt(jnp.mean(mixed * mixed, axis=-1, keepdims=True) + 1e-06) * out_gain
    return normed.astype(jnp.bfloat16)


def solution(mesh):
    placed = (
        P(("dp", "kv"), None),
        P(("dp", "kv"), None),
        P("kv", "tp"),
        P("kv", "tp"),
        P("kv", "tp"),
        P("tp", "kv"),
        P(),
    )
    n_dp, n_kv, n_tp = (mesh.shape[name] for name in ("dp", "kv", "tp"))

    def body(tokens, chosen, query_weight, key_matrix, value_matrix, out_weight, out_gain):
        args = (tokens, chosen, query_weight, key_matrix, value_matrix, out_weight, out_gain)
        depth, columns = query_weight.shape
        whole_tiles = (
            depth % (LANES * n_dp) == 0
            and depth % (32 * PIECES[1] * n_dp) == 0
            and out_weight.shape[0] % (32 * PIECES[2] * n_dp) == 0
            and out_weight.shape[1] % LANES == 0
            and columns % LANES == 0
            and key_matrix.shape[1] == HEAD_WIDTH
            and chosen.shape[1] % 2 == 0
            and n_tp == 2
            and n_dp == 4
            and n_kv == 4
            and tokens.shape[0] == 8 * BLOCK_LENGTH
        )
        if whole_tiles:
            return per_device_fused(n_dp, n_kv, n_tp, *args)
        return per_device(*args)

    return jax.shard_map(
        body,
        mesh=mesh,
        in_specs=placed,
        out_specs=P(("dp", "kv", "tp"), None),
        check_vma=False,
    )
```

```python
import functools

import jax
import jax.numpy as jnp
from jax import lax
from jax.experimental import pallas as pl
from jax.experimental.pallas import tpu as pltpu
from jax.sharding import PartitionSpec as P

HEAD_WIDTH = 64
BLOCK_LENGTH = 64
LANES = 2 * HEAD_WIDTH
HIDDEN = -1e30
CAP = 2
PIECES = (1, 2, 2)


def remote(src, dst, send, recv, axis, peer):
    return pltpu.make_async_remote_copy(
        src_ref=src,
        dst_ref=dst,
        send_sem=send,
        recv_sem=recv,
        device_id={axis: peer},
        device_id_type=pl.DeviceIdType.MESH,
    )


def fused(
    n_dp, n_kv, n_tp,
    chosen_hbm, tokens_hbm, key_hbm, value_hbm, query_hbm, out_hbm, gain_hbm, result,
    chosen, spots, lowest_of, gain, tokens, pair_own, query_own, out_own, wanted, asks, packed, kv_own, kv_far,
    pair_all, query_all, out_all, kv_all, query_sum, query_rows, attended,
    leaving, arriving, kept,
    load_sem, z_send, z_recv, d_send, d_recv, r_send, r_recv, kv_send, kv_recv, t_send, t_recv, ask_send, ask_recv,
):
    d, z, t = lax.axis_index("dp"), lax.axis_index("kv"), lax.axis_index("tp")
    rows, width = tokens.shape
    blocks = rows // BLOCK_LENGTH
    depth = width // n_kv
    half = rows // n_tp
    cut = depth // n_dp
    loads = [
        pltpu.make_async_copy(source, target, load_sem.at[k])
        for k, (source, target) in enumerate(
            ((query_hbm, query_own), (tokens_hbm, tokens), (out_hbm, out_own),
             (gain_hbm, gain), (chosen_hbm, wanted), (chosen_hbm, chosen))
        )
    ]
    pair_loads = [
        pltpu.make_async_copy(
            source.at[:, k * cut : (k + 1) * cut],
            pair_own.at[k, side * HEAD_WIDTH : (side + 1) * HEAD_WIDTH],
            load_sem.at[6],
        )
        for k in range(n_dp)
        for side, source in enumerate((key_hbm, value_hbm))
    ]
    for load in pair_loads + loads:
        load.start()

    barrier = pltpu.get_barrier_semaphore()
    for axis, me, count in (("dp", d, n_dp), ("kv", z, n_kv), ("tp", t, n_tp)):
        for step in range(1, count):
            pl.semaphore_signal(
                barrier, inc=1, device_id={axis: lax.rem(me + step, count)},
                device_id_type=pl.DeviceIdType.MESH,
            )
    pl.semaphore_wait(barrier, n_dp + n_kv + n_tp - 3)

    owns = (pair_own, query_own, out_own)
    alls = (pair_all, query_all, out_all)
    events = [
        (which, part, j) for which in range(3) for part in range(PIECES[which]) for j in range(1, n_kv)
    ]
    origin = (z, z + 1 - 2 * lax.rem(z, 2), lax.rem(z + 2, 4), 3 - z)
    middle = (z == 1) | (z == 2)
    near = (d, d + 1 - 2 * lax.rem(d, 2), lax.rem(d + 2, 4))
    corner = 3 - d

    def span_of(e, share=0, shares=1):
        which, part, _ = events[e]
        size = owns[which].shape[1] // PIECES[which]
        return pl.ds(part * size + share * (size // shares), size // shares)

    def first(e):
        which, _, j = events[e]
        return remote(
            owns[which].at[d, span_of(e)], alls[which].at[z, d, span_of(e)],
            z_send.at[which], z_recv.at[e], "kv", origin[j],
        )

    def first_in(e):
        which, _, j = events[e]
        slot = alls[which].at[origin[j], d, span_of(e)]
        return remote(slot, slot, z_send.at[which], z_recv.at[e], "kv", origin[j])

    def onward(e):
        which, _, j = events[e]
        slot = alls[which].at[origin[j], d, span_of(e)]
        return remote(slot, slot, z_send.at[which], z_recv.at[e + 1], "kv", origin[1])

    def second(e, k):
        which, _, j = events[e]
        slot = alls[which].at[origin[j], d, span_of(e)]
        return remote(slot, slot, d_send.at[which], d_recv.at[e], "dp", near[k])

    def second_in(e):
        which, _, j = events[e]
        slots = alls[which].at[origin[j], 0:2, span_of(e)]
        return remote(slots, slots, d_send.at[which], d_recv.at[e], "dp", near[1])

    def halfway(e, k):
        which, _, j = events[e]
        slot = alls[which].at[origin[j], near[k], span_of(e, k - 1, 2)]
        return remote(slot, slot, r_send.at[which], r_recv.at[e], "dp", near[3 - k])

    def halfway_in(e):
        which, _, j = events[e]
        slot = alls[which].at[origin[j], corner, span_of(e)]
        return remote(slot, slot, r_send.at[which], r_recv.at[e], "dp", near[1])

    def out(e):
        if events[e][2] == 3:

            @pl.when(middle)
            def _():
                first(e).start()
        else:
            first(e).start()

    def pass_on(e):
        first_in(e).wait_recv()
        if events[e][2] == 2:

            @pl.when(middle)
            def _():
                onward(e).start()

        for k in (1, 2):
            second(e, k).start()

    def relay(e):
        second_in(e).wait_recv()
        for k in (1, 2):
            halfway(e, k).start()

    def take(e):
        halfway_in(e).wait_recv()

    def whole(which, j):
        block = owns[which][...] if j == 0 else alls[which][origin[j]]
        return block.reshape(block.shape[0] * block.shape[1], block.shape[2])

    def token_part(j):
        start = pl.multiple_of(origin[j] * depth, depth)
        return tokens[:, pl.ds(start, depth)]

    def ask(j):
        return remote(wanted, asks.at[z], ask_send.at[0], ask_recv.at[0], "kv", origin[j])

    def asks_in():
        slots = asks.at[0 : n_kv - 1]
        return remote(slots, slots, ask_send.at[0], ask_recv.at[0], "kv", origin[1])

    loads[4].wait()
    for j in range(1, n_kv):
        ask(j).start()
    pltpu.make_async_copy(pair_own, pair_own, load_sem.at[6]).wait()
    for e in (1, 0):
        out(e)
    loads[0].wait()
    for e in (3, 4):
        out(e)
    pass_on(0)
    out(2)
    pass_on(1)
    out(7)
    pass_on(3)
    for e in (6, 5, 8):
        out(e)
    loads[2].wait()
    out(13)
    relay(0)
    pass_on(2)
    relay(1)
    pass_on(4)
    out(10)
    relay(3)
    out(9)
    take(0)
    relay(2)
    for e in (7, 6):
        pass_on(e)
    take(1)
    out(12)
    take(2)
    pass_on(5)
    for load in loads[1:2] + loads[3:4] + loads[5:]:
        load.wait()

    def pair_part(j):
        block = pair_own[...] if j == 0 else pair_all[origin[j]]
        block = jnp.concatenate([block[k] for k in range(n_dp)], axis=1)
        return lax.dot_general(
            token_part(j), block, (((1,), (1,)), ((), ())), preferred_element_type=jnp.float32
        )

    total = pair_part(0)
    for j in range(1, n_kv):
        total += pair_part(j)
    kv_own[...] = total.astype(jnp.bfloat16).reshape(blocks, BLOCK_LENGTH, LANES)

    def named(rows_of, owner):
        local = rows_of - owner * blocks
        inside = (local >= 0) & (local < blocks)
        return (
            jnp.min(jnp.where(inside, local, blocks - 1)),
            jnp.max(jnp.where(inside, local, 0)),
        )

    def kv_out(j):
        return remote(
            packed.at[j], kv_far.at[pl.ds(z * CAP, CAP)], kv_send.at[0], kv_recv.at[0],
            "kv", origin[j],
        )

    def kv_in():
        slots = kv_far.at[0 : (n_kv - 1) * CAP]
        return remote(slots, slots, kv_send.at[0], kv_recv.at[0], "kv", origin[1])

    kv_far[pl.ds(z * CAP, CAP)] = jnp.zeros((CAP, BLOCK_LENGTH, LANES), jnp.bfloat16)
    asks_in().wait_recv()
    for j in range(1, n_kv):
        lowest, highest = named(asks[origin[j]], z)
        packed[j, 0] = kv_own[lowest]
        packed[j, 1] = kv_own[highest]
    picks = chosen.shape[1]
    for owner in range(n_kv):
        lowest_of[owner] = named(wanted[...], owner)[0] + owner * blocks
    pass_on(8)
    for e in (7, 6):
        relay(e)
    for j in range(1, n_kv):
        kv_out(j).start()

    def locate(b, carry):
        for s in range(picks):
            name = jnp.maximum(chosen[b, s], 0)
            owner = lax.div(name, blocks)
            far = owner * CAP + jnp.where(name == lowest_of[owner], 0, 1)
            spots[b, s] = jnp.where(owner == z, name - z * blocks + n_kv * CAP, far)
        return carry

    lax.fori_loop(0, blocks, locate, 0)
    relay(4)
    take(3)
    relay(5)
    query_sum[...] = jnp.dot(token_part(0), whole(1, 0), preferred_element_type=jnp.float32)
    relay(8)
    take(7)
    for e in (13, 9, 12):
        pass_on(e)
    out(14)
    take(6)
    out(11)
    take(4)
    query_sum[...] += jnp.dot(
        token_part(1), whole(1, 1), preferred_element_type=jnp.float32
    )
    pass_on(10)
    take(5)
    query_sum[...] += jnp.dot(
        token_part(2), whole(1, 2), preferred_element_type=jnp.float32
    )
    take(8)
    query_sum[...] += jnp.dot(
        token_part(3), whole(1, 3), preferred_element_type=jnp.float32
    )
    low_half = lax.broadcasted_iota(jnp.int32, (rows, LANES), 1) < HEAD_WIDTH
    for p in range(query_sum.shape[1] // LANES):
        both = query_sum[:, p * LANES : (p + 1) * LANES]
        for side, one in enumerate((both, pltpu.roll(both, HEAD_WIDTH, 1))):
            one = jnp.where(low_half, one, 0.0).astype(jnp.bfloat16)
            query_rows[2 * p + side] = one * jnp.bfloat16(HEAD_WIDTH ** (-0.5))
    kv_in().wait_recv()

    kv_all[0 : n_kv * CAP] = kv_far[...]
    kv_all[n_kv * CAP :] = kv_own[...]

    pass_on(14)

    heads = query_rows.shape[0]
    group = heads // 2

    def attend(b, carry):
        @pl.when(b == 2)
        def _():
            pass_on(11)
            relay(9)

        @pl.when(b == 4)
        def _():
            for e in (12, 13):
                relay(e)

        @pl.when(b == 5)
        def _():
            for e in (14, 10):
                relay(e)

        @pl.when(b == 6)
        def _():
            relay(11)

        lane = lax.broadcasted_iota(jnp.int32, (BLOCK_LENGTH, LANES), 1)
        row = lax.broadcasted_iota(jnp.int32, (BLOCK_LENGTH, LANES), 0)
        low = lane < HEAD_WIDTH
        offs = [jnp.where(chosen[b, s] >= 0, 0.0, HIDDEN) for s in range(picks)]
        bias = []
        for s in range(0, picks, 2):
            tile = jnp.where(low, offs[s], offs[s + 1])
            if s == 0:
                tile = jnp.where(low & (lane > row), HIDDEN, tile)
            bias.append(tile)
        bias = jnp.concatenate(bias, axis=1)
        kv = jnp.concatenate([kv_all[spots[b, s]] for s in range(picks)], axis=0)
        at = pl.ds(pl.multiple_of(b * BLOCK_LENGTH, BLOCK_LENGTH), BLOCK_LENGTH)

        def score(start):
            query = query_rows[start : start + group, at, :].reshape(group * BLOCK_LENGTH, LANES)
            return lax.dot_general(
                query, kv, (((1,), (1,)), ((), ())), preferred_element_type=jnp.float32
            )

        outs = []
        later = score(0)
        for start in range(0, heads, group):
            scores = later.reshape(group, BLOCK_LENGTH, picks * BLOCK_LENGTH) + bias[None]
            if start + group < heads:
                later = score(start + group)
            top = jnp.max(scores, axis=2, keepdims=True)
            expon = jnp.exp(scores - top)
            inverse = 1.0 / jnp.sum(expon, axis=2, keepdims=True)
            probs = expon.astype(jnp.bfloat16).reshape(group * BLOCK_LENGTH, picks * BLOCK_LENGTH)
            out_rows = jnp.dot(probs, kv, preferred_element_type=jnp.float32)
            out_rows = out_rows.reshape(group, BLOCK_LENGTH, LANES) * inverse
            outs += [out_rows[h] for h in range(group)]
        for p in range(heads // 2):
            joined = jnp.where(low, pltpu.roll(outs[2 * p], HEAD_WIDTH, 1), outs[2 * p + 1])
            attended[at, p * LANES : (p + 1) * LANES] = joined.astype(jnp.bfloat16)
        return carry

    lax.fori_loop(0, blocks, attend, 0)

    peer = lax.rem(t + 1, n_tp)
    other_rows = attended[pl.ds(pl.multiple_of(peer * half, half), half), :]
    own_rows = attended[pl.ds(pl.multiple_of(t * half, half), half), :]

    def swap_half(j):
        return remote(
            leaving.at[origin[j]], arriving.at[origin[j]], t_send.at[0], t_recv.at[j], "tp", peer
        )

    def project(j):
        weight = whole(2, j)
        leaving[origin[j]] = jnp.dot(
            other_rows, weight, preferred_element_type=jnp.float32
        ).astype(jnp.bfloat16)
        swap_half(j).start()
        kept[origin[j]] = jnp.dot(own_rows, weight, preferred_element_type=jnp.float32)

    for e in (13, 9):
        take(e)
    project(0)
    take(12)
    project(1)
    take(10)
    project(2)
    for e in (11, 14):
        take(e)
    project(3)

    square = jnp.zeros((half, 1), jnp.float32)
    for j in range(n_kv):
        slot = origin[j]
        swap_half(j).wait_recv()
        mixed = kept[slot] + arriving[slot].astype(jnp.float32)
        kept[slot] = mixed
        square += jnp.sum(mixed * mixed, axis=1, keepdims=True)
    scale = lax.rsqrt(square * (1.0 / width) + 1e-06)
    for j in range(n_kv):
        columns = slice(j * depth, (j + 1) * depth)
        result[:, columns] = (kept[j] * scale * gain[:, columns]).astype(jnp.bfloat16)

    def drain(slots, sem):
        remote(slots, slots, sem, z_recv.at[0], "kv", origin[1]).wait_send()

    for which in range(3):
        drain(alls[which].at[0 : n_kv - 1, 0:2], d_send.at[which])
        drain(alls[which].at[0 : n_kv - 1, 0], r_send.at[which])

    @pl.when(middle)
    def _():
        for which in range(3):
            drain(alls[which].at[:, 0], z_send.at[which])

    @pl.when(jnp.logical_not(middle))
    def _():
        for which in range(3):
            drain(alls[which].at[0:2, 0], z_send.at[which])

    drain(packed.at[1:n_kv], kv_send.at[0])
    drain(asks.at[0 : n_kv - 1], ask_send.at[0])
    drain(leaving, t_send.at[0])


def per_device_fused(
    n_dp, n_kv, n_tp,
    tokens, chosen, query_weight, key_matrix, value_matrix, out_weight, out_gain,
):
    rows, width = tokens.shape
    depth, columns = query_weight.shape
    blocks = rows // BLOCK_LENGTH
    cut = lambda w: w.reshape(n_dp, w.shape[0] // n_dp, w.shape[1])
    query, out = cut(query_weight), cut(out_weight)
    pair = jax.ShapeDtypeStruct((n_dp, LANES, depth // n_dp), jnp.bfloat16)
    bf16, f32 = jnp.bfloat16, jnp.float32
    vmem = pl.BlockSpec(memory_space=pltpu.VMEM)
    off_core = pl.BlockSpec(memory_space=pltpu.HBM)
    dma = pltpu.SemaphoreType.DMA
    copies = sum(PIECES) * (n_kv - 1)
    return pl.pallas_call(
        functools.partial(fused, n_dp, n_kv, n_tp),
        out_shape=pltpu.VMEM((rows // n_tp, width), bf16),
        in_specs=[
            off_core, off_core, off_core, off_core, off_core, off_core, off_core,
        ],
        out_specs=vmem,
        scratch_shapes=[
            pltpu.SMEM((blocks, chosen.shape[1]), jnp.int32),
            pltpu.SMEM((blocks, chosen.shape[1]), jnp.int32),
            pltpu.SMEM((n_kv,), jnp.int32),
            pltpu.VMEM((1, width), f32),
            pltpu.VMEM((rows, width), bf16),
            pltpu.VMEM(pair.shape, bf16),
            pltpu.VMEM(query.shape, bf16),
            pltpu.VMEM(out.shape, bf16),
            pltpu.VMEM((blocks, chosen.shape[1]), jnp.int32),
            pltpu.VMEM((n_kv, blocks, chosen.shape[1]), jnp.int32),
            pltpu.VMEM((n_kv, CAP, BLOCK_LENGTH, LANES), bf16),
            pltpu.VMEM((blocks, BLOCK_LENGTH, LANES), bf16),
            pltpu.VMEM((n_kv * CAP, BLOCK_LENGTH, LANES), bf16),
            pltpu.VMEM((n_kv,) + pair.shape, bf16),
            pltpu.VMEM((n_kv,) + query.shape, bf16),
            pltpu.VMEM((n_kv,) + out.shape, bf16),
            pltpu.VMEM((n_kv * CAP + blocks, BLOCK_LENGTH, LANES), bf16),
            pltpu.VMEM((rows, columns), f32),
            pltpu.VMEM((columns // HEAD_WIDTH, rows, LANES), bf16),
            pltpu.VMEM((rows, columns), bf16),
            pltpu.VMEM((n_kv, rows // n_tp, width // n_kv), bf16),
            pltpu.VMEM((n_kv, rows // n_tp, width // n_kv), bf16),
            pltpu.VMEM((n_kv, rows // n_tp, width // n_kv), f32),
            dma((7,)), dma((3,)), dma((copies,)), dma((3,)), dma((copies,)), dma((3,)), dma((copies,)),
            dma((1,)), dma((1,)), dma((1,)), dma((n_kv,)), dma((1,)), dma((1,)),
        ],
        compiler_params=pltpu.CompilerParams(
            collective_id=0, has_side_effects=True, vmem_limit_bytes=54 * 1024 * 1024
        ),
    )(chosen, tokens, key_matrix.T, value_matrix.T, query, out, out_gain.reshape(1, width))


def per_device(tokens, chosen, query_weight, key_matrix, value_matrix, out_weight, out_gain):
    tok_rows = tokens.shape[0]
    blocks = tok_rows // BLOCK_LENGTH
    device = lax.axis_index("kv")
    kv_count = lax.axis_size("kv")
    whole_query, whole_key, whole_value = (
        lax.all_gather(query_weight, "kv", axis=0, tiled=True),
        lax.all_gather(key_matrix, "kv", axis=0, tiled=True),
        lax.all_gather(value_matrix, "kv", axis=0, tiled=True),
    )
    query_rows = jnp.dot(tokens, whole_query, preferred_element_type=jnp.float32).astype(
        jnp.bfloat16
    )
    key_rows = jnp.dot(tokens, whole_key, preferred_element_type=jnp.float32).astype(jnp.bfloat16)
    value_rows = jnp.dot(tokens, whole_value, preferred_element_type=jnp.float32).astype(
        jnp.bfloat16
    )
    paired = jnp.concatenate([key_rows, value_rows], axis=1)
    pair_width = paired.shape[1]
    safe_ids = jnp.maximum(chosen, 0)
    everyone = lax.all_gather(paired, "kv", axis=0, tiled=True).reshape(
        kv_count * blocks, BLOCK_LENGTH, pair_width
    )
    picked = jnp.take(everyone, safe_ids, axis=0)
    head_count = query_rows.shape[1] // HEAD_WIDTH
    grouped = query_rows.reshape(blocks, BLOCK_LENGTH, head_count, HEAD_WIDTH)
    offsets = jnp.arange(BLOCK_LENGTH, dtype=jnp.int32)
    query_pos = (device * blocks + jnp.arange(blocks, dtype=jnp.int32))[
        :, None
    ] * BLOCK_LENGTH + offsets[None, :]
    key_pos = safe_ids[:, :, None] * BLOCK_LENGTH + offsets[None, None, :]
    visible = (chosen >= 0)[:, None, :, None] & (
        key_pos[:, None, :, :] <= query_pos[:, :, None, None]
    )

    def attend_block(inputs):
        query_block, pair_block, seen = inputs
        block_keys = pair_block[..., :HEAD_WIDTH]
        block_values = pair_block[..., HEAD_WIDTH:]
        scores = jnp.einsum(
            "qgd,skd->gqsk", query_block, block_keys, preferred_element_type=jnp.float32
        ) * HEAD_WIDTH ** (-0.5)
        scores = jnp.where(seen[None], scores, -1e30)
        row_max = jnp.max(scores, axis=(2, 3), keepdims=True)
        expon = jnp.exp(scores - row_max)
        row_sum = jnp.sum(expon, axis=(2, 3), keepdims=True)
        weights_bf = (expon / row_sum).astype(jnp.bfloat16)
        result = jnp.einsum(
            "gqsk,skd->qgd", weights_bf, block_values, preferred_element_type=jnp.float32
        )
        return result.astype(jnp.bfloat16)

    attended = lax.map(attend_block, (grouped, picked, visible))
    attended = attended.reshape(tok_rows, head_count * HEAD_WIDTH)
    whole_out = lax.all_gather(out_weight, "kv", axis=1, tiled=True)
    mixed = lax.psum_scatter(
        jnp.dot(attended, whole_out, preferred_element_type=jnp.float32).astype(jnp.bfloat16),
        "tp",
        scatter_dimension=0,
        tiled=True,
    ).astype(jnp.float32)
    normed = mixed * lax.rsqrt(jnp.mean(mixed * mixed, axis=-1, keepdims=True) + 1e-06) * out_gain
    return normed.astype(jnp.bfloat16)


def solution(mesh):
    placed = (
        P(("dp", "kv"), None),
        P(("dp", "kv"), None),
        P("kv", "tp"),
        P("kv", "tp"),
        P("kv", "tp"),
        P("tp", "kv"),
        P(),
    )
    n_dp, n_kv, n_tp = (mesh.shape[name] for name in ("dp", "kv", "tp"))

    def body(tokens, chosen, query_weight, key_matrix, value_matrix, out_weight, out_gain):
        args = (tokens, chosen, query_weight, key_matrix, value_matrix, out_weight, out_gain)
        depth, columns = query_weight.shape
        whole_tiles = (
            depth % (LANES * n_dp) == 0
            and depth % (32 * PIECES[1] * n_dp) == 0
            and out_weight.shape[0] % (32 * PIECES[2] * n_dp) == 0
            and out_weight.shape[1] % LANES == 0
            and columns % LANES == 0
            and key_matrix.shape[1] == HEAD_WIDTH
            and chosen.shape[1] % 2 == 0
            and n_tp == 2
            and n_dp == 4
            and n_kv == 4
            and tokens.shape[0] == 8 * BLOCK_LENGTH
        )
        if whole_tiles:
            return per_device_fused(n_dp, n_kv, n_tp, *args)
        return per_device(*args)

    return jax.shard_map(
        body,
        mesh=mesh,
        in_specs=placed,
        out_specs=P(("dp", "kv", "tp"), None),
        check_vma=False,
    )
```

```python
import functools

import jax
import jax.numpy as jnp
from jax import lax
from jax.experimental import pallas as pl
from jax.experimental.pallas import tpu as pltpu
from jax.sharding import PartitionSpec as P

HEAD_WIDTH = 64
BLOCK_LENGTH = 64
LANES = 2 * HEAD_WIDTH
HIDDEN = -1e30
CAP = 2
PIECES = (1, 2, 2)
FAR = 1


def remote(src, dst, send, recv, axis, peer):
    return pltpu.make_async_remote_copy(
        src_ref=src,
        dst_ref=dst,
        send_sem=send,
        recv_sem=recv,
        device_id={axis: peer},
        device_id_type=pl.DeviceIdType.MESH,
    )


def fused(
    n_dp, n_kv, n_tp,
    chosen_hbm, tokens_hbm, key_hbm, value_hbm, query_hbm, out_hbm, gain_hbm, result,
    chosen, spots, lowest_of, gain, tokens, pair_own, query_own, out_own, wanted, asks, packed, kv_own, kv_far,
    pair_all, query_all, out_all, kv_all, query_sum, query_rows, attended,
    leaving, arriving, kept,
    load_sem, z_send, z_recv, c_send, c_recv, d_send, d_recv, r_send, r_recv, kv_send, kv_recv, t_send, t_recv, ask_send, ask_recv,
):
    d, z, t = lax.axis_index("dp"), lax.axis_index("kv"), lax.axis_index("tp")
    rows, width = tokens.shape
    blocks = rows // BLOCK_LENGTH
    depth = width // n_kv
    half = rows // n_tp
    cut = depth // n_dp
    loads = [
        pltpu.make_async_copy(source, target, load_sem.at[k])
        for k, (source, target) in enumerate(
            ((tokens_hbm, tokens), (out_hbm, out_own), (gain_hbm, gain), (chosen_hbm, wanted),
             (chosen_hbm, chosen))
        )
    ]
    part_width = query_own.shape[3]
    query_loads = [
        pltpu.make_async_copy(
            query_hbm.at[:, :, part * part_width : (part + 1) * part_width], query_own.at[part],
            load_sem.at[6 + part],
        )
        for part in range(PIECES[1])
    ]
    pair_loads = [
        pltpu.make_async_copy(
            source.at[:, k * cut : (k + 1) * cut],
            pair_own.at[k, side * HEAD_WIDTH : (side + 1) * HEAD_WIDTH],
            load_sem.at[5],
        )
        for k in range(n_dp)
        for side, source in enumerate((key_hbm, value_hbm))
    ]
    for load in pair_loads + loads[3:4] + query_loads + loads[:3] + loads[4:]:
        load.start()

    barrier = pltpu.get_barrier_semaphore()
    for axis, me, count in (("dp", d, n_dp), ("kv", z, n_kv), ("tp", t, n_tp)):
        for step in range(1, count):
            pl.semaphore_signal(
                barrier, inc=1, device_id={axis: lax.rem(me + step, count)},
                device_id_type=pl.DeviceIdType.MESH,
            )
    pl.semaphore_wait(barrier, n_dp + n_kv + n_tp - 3)

    owns = (pair_own, query_own, out_own)
    alls = (pair_all, query_all, out_all)
    events = [
        (which, part, j) for which in range(3) for part in range(PIECES[which]) for j in range(1, n_kv)
    ]
    far = [e for e, event in enumerate(events) if event[0] == 2 and event[1] >= PIECES[2] - FAR]
    origin = (z, z + 1 - 2 * lax.rem(z, 2), lax.rem(z + 2, 4), 3 - z)
    middle = (z == 1) | (z == 2)
    near = (d, d + 1 - 2 * lax.rem(d, 2), lax.rem(d + 2, 4))
    corner = 3 - d

    def piece_of(e, planes, plane, quarter, share=0, shares=1):
        which, part, _ = events[e]
        lead = (plane,) if planes else ()
        refs = alls if planes else owns
        if which == 1:
            size = refs[which].shape[-2] // shares
            return refs[which].at[(*lead, part, quarter, pl.ds(share * size, size))]
        size = refs[which].shape[-2] // PIECES[which]
        span = pl.ds(part * size + share * (size // shares), size // shares)
        return refs[which].at[(*lead, quarter, span)]

    def slot(e, quarter, share=0, shares=1):
        return piece_of(e, True, origin[events[e][2]], quarter, share, shares)

    def across(e, quarter, send, recv):
        return remote(
            piece_of(e, False, None, quarter), piece_of(e, True, z, quarter), send, recv,
            "kv", origin[events[e][2]],
        )

    def first(e):
        return across(e, d, z_send.at[events[e][0]], z_recv.at[e])

    def first_far(e):
        return across(e, corner, c_send.at[0], c_recv.at[far.index(e)])

    def landed(e, quarter, recv):
        place = slot(e, quarter)
        return remote(place, place, c_send.at[0], recv, "kv", origin[1])

    def onward(e):
        place = slot(e, d)
        return remote(place, place, z_send.at[events[e][0]], z_recv.at[e + 1], "kv", origin[1])

    def onward_far(e):
        place = slot(e, corner)
        return remote(
            place, place, c_send.at[0], c_recv.at[far.index(e) + 1], "kv", origin[1]
        )

    def second(e, k):
        place = slot(e, d)
        return remote(place, place, d_send.at[events[e][0]], d_recv.at[e], "dp", near[k])

    def second_in(e):
        places = slot(e, pl.ds(0, 2))
        return remote(places, places, d_send.at[events[e][0]], d_recv.at[e], "dp", near[1])

    def halfway(e, k):
        place = slot(e, near[k], k - 1, 2)
        return remote(place, place, r_send.at[events[e][0]], r_recv.at[e], "dp", near[3 - k])

    def halfway_in(e):
        place = slot(e, corner)
        return remote(place, place, r_send.at[events[e][0]], r_recv.at[e], "dp", near[1])

    def begin(copy, e):
        if events[e][2] == 3:

            @pl.when(middle)
            def _():
                copy(e).start()
        else:
            copy(e).start()

    def hand_on(copy, e):
        if events[e][2] == 2:

            @pl.when(middle)
            def _():
                copy(e).start()

    def out(e):
        begin(first, e)

    def out_far(e):
        begin(first_far, e)

    def pass_on(e):
        landed(e, d, z_recv.at[e]).wait_recv()
        hand_on(onward, e)
        for k in (1, 2):
            second(e, k).start()

    def pass_far(e):
        landed(e, corner, c_recv.at[far.index(e)]).wait_recv()
        hand_on(onward_far, e)

    def relay(e):
        second_in(e).wait_recv()
        if e not in far:
            for k in (1, 2):
                halfway(e, k).start()

    def take(e):
        halfway_in(e).wait_recv()

    def whole(which, j, part=None):
        block = owns[which] if j == 0 else alls[which].at[origin[j]]
        block = block[...] if part is None else block[part]
        return block.reshape(block.shape[0] * block.shape[1], block.shape[2])

    def token_part(j):
        start = pl.multiple_of(origin[j] * depth, depth)
        return tokens[:, pl.ds(start, depth)]

    def ask(j):
        return remote(wanted, asks.at[z], ask_send.at[0], ask_recv.at[0], "kv", origin[j])

    def asks_in():
        slots = asks.at[0 : n_kv - 1]
        return remote(slots, slots, ask_send.at[0], ask_recv.at[0], "kv", origin[1])

    def pair_part(j):
        block = pair_own[...] if j == 0 else pair_all[origin[j]]
        block = jnp.concatenate([block[k] for k in range(n_dp)], axis=1)
        return lax.dot_general(
            token_part(j), block, (((1,), (1,)), ((), ())), preferred_element_type=jnp.float32
        )

    def pair_stage():
        total = pair_part(0)
        for j in range(1, n_kv):
            total += pair_part(j)
        kv_own[...] = total.astype(jnp.bfloat16).reshape(blocks, BLOCK_LENGTH, LANES)

    def named(rows_of, owner):
        local = rows_of - owner * blocks
        inside = (local >= 0) & (local < blocks)
        return (
            jnp.min(jnp.where(inside, local, blocks - 1)),
            jnp.max(jnp.where(inside, local, 0)),
        )

    def kv_out(j):
        return remote(
            packed.at[j], kv_far.at[pl.ds(z * CAP, CAP)], kv_send.at[0], kv_recv.at[0],
            "kv", origin[j],
        )

    def kv_in():
        slots = kv_far.at[0 : (n_kv - 1) * CAP]
        return remote(slots, slots, kv_send.at[0], kv_recv.at[0], "kv", origin[1])

    picks = chosen.shape[1]

    def locate(b, carry):
        for s in range(picks):
            name = jnp.maximum(chosen[b, s], 0)
            owner = lax.div(name, blocks)
            far = owner * CAP + jnp.where(name == lowest_of[owner], 0, 1)
            spots[b, s] = jnp.where(owner == z, name - z * blocks + n_kv * CAP, far)
        return carry

    def share_blocks():
        kv_far[pl.ds(z * CAP, CAP)] = jnp.zeros((CAP, BLOCK_LENGTH, LANES), jnp.bfloat16)
        asks_in().wait_recv()
        for j in range(1, n_kv):
            lowest, highest = named(asks[origin[j]], z)
            packed[j, 0] = kv_own[lowest]
            packed[j, 1] = kv_own[highest]
        for owner in range(n_kv):
            lowest_of[owner] = named(wanted[...], owner)[0] + owner * blocks
        for j in range(1, n_kv):
            kv_out(j).start()
        lax.fori_loop(0, blocks, locate, 0)

    def query_part(part, j):
        term = jnp.dot(
            token_part(j), whole(1, j, part), preferred_element_type=jnp.float32
        )
        query_sum[...] = term if j == 0 else query_sum[...] + term

    heads = query_rows.shape[0]
    group = heads // PIECES[1]

    def query_tiles(part):
        low_half = lax.broadcasted_iota(jnp.int32, (rows, LANES), 1) < HEAD_WIDTH
        for p in range(group // 2):
            both = query_sum[:, p * LANES : (p + 1) * LANES]
            for side, one in enumerate((both, pltpu.roll(both, HEAD_WIDTH, 1))):
                one = jnp.where(low_half, one, 0.0).astype(jnp.bfloat16)
                one = one * jnp.bfloat16(HEAD_WIDTH ** (-0.5))
                query_rows[part * group + 2 * p + side] = one

    def gather_blocks():
        kv_in().wait_recv()
        kv_all[0 : n_kv * CAP] = kv_far[...]
        kv_all[n_kv * CAP :] = kv_own[...]

    lane = lax.broadcasted_iota(jnp.int32, (BLOCK_LENGTH, LANES), 1)
    row = lax.broadcasted_iota(jnp.int32, (BLOCK_LENGTH, LANES), 0)
    low = lane < HEAD_WIDTH

    def attend(part, start, count):
        def score(b):
            kv = jnp.concatenate([kv_all[spots[b, s]] for s in range(picks)], axis=0)
            query = query_rows[
                part * group : (part + 1) * group, b * BLOCK_LENGTH : (b + 1) * BLOCK_LENGTH, :
            ].reshape(group * BLOCK_LENGTH, LANES)
            scores = lax.dot_general(
                query, kv, (((1,), (1,)), ((), ())), preferred_element_type=jnp.float32
            )
            return kv, scores

        later = score(start)
        for b in range(start, start + count):
            kv, scores = later
            if b + 1 < start + count:
                later = score(b + 1)
            offs = [jnp.where(chosen[b, s] >= 0, 0.0, HIDDEN) for s in range(picks)]
            bias = []
            for s in range(0, picks, 2):
                tile = jnp.where(low, offs[s], offs[s + 1])
                if s == 0:
                    tile = jnp.where(low & (lane > row), HIDDEN, tile)
                bias.append(tile)
            bias = jnp.concatenate(bias, axis=1)
            scores = scores.reshape(group, BLOCK_LENGTH, picks * BLOCK_LENGTH) + bias[None]
            top = jnp.max(scores, axis=2, keepdims=True)
            expon = jnp.exp(scores - top)
            inverse = 1.0 / jnp.sum(expon, axis=2, keepdims=True)
            probs = expon.astype(jnp.bfloat16).reshape(group * BLOCK_LENGTH, picks * BLOCK_LENGTH)
            mixed = jnp.dot(probs, kv, preferred_element_type=jnp.float32)
            mixed = mixed.reshape(group, BLOCK_LENGTH, LANES) * inverse
            for p in range(group // 2):
                joined = jnp.where(low, pltpu.roll(mixed[2 * p], HEAD_WIDTH, 1), mixed[2 * p + 1])
                column = (part * group // 2 + p) * LANES
                attended[b * BLOCK_LENGTH : (b + 1) * BLOCK_LENGTH, column : column + LANES] = (
                    joined.astype(jnp.bfloat16)
                )

    loads[3].wait()
    for j in range(1, n_kv):
        ask(j).start()
    pltpu.make_async_copy(pair_own, pair_own, load_sem.at[5]).wait()
    out(1)
    query_loads[1].wait()
    for e in (6, 2, 0):
        out(e)
    query_loads[0].wait()
    for e in (4, 5):
        out(e)
    for e in (1, 6, 0):
        pass_on(e)
    out(3)
    pass_on(2)
    out(7)
    pass_on(4)
    relay(0)
    pass_on(3)
    relay(1)
    loads[1].wait()
    for e in (10, 12, 8):
        out(e)
    relay(2)
    out(13)
    relay(4)
    for e in (5, 7):
        pass_on(e)
    take(1)
    relay(3)
    for e in (0, 2):
        take(e)
    loads[0].wait()
    query_part(0, 0)
    pair_stage()
    loads[4].wait()
    share_blocks()
    for e in (5, 6):
        relay(e)
    pass_on(8)
    out(9)
    relay(7)
    for e in (10, 13):
        pass_on(e)
    take(3)
    query_part(0, 1)
    out(11)
    take(4)
    out(14)
    take(5)
    query_part(0, 2)
    query_part(0, 3)
    take(6)
    out_far(12)
    query_tiles(0)
    query_part(1, 0)
    query_part(1, 1)
    out_far(13)
    relay(8)
    gather_blocks()
    pass_on(9)
    attend(0, blocks * 0 // 2, blocks // 2)
    take(7)
    pass_on(11)
    attend(0, blocks * 1 // 2, blocks // 2)
    relay(10)
    query_part(1, 2)
    take(8)
    pass_on(12)
    query_part(1, 3)
    out_far(14)
    pass_far(12)
    query_tiles(1)
    relay(9)
    pass_far(13)
    pass_on(14)
    relay(13)
    attend(1, blocks * 0 // 2, blocks // 2)
    relay(11)
    attend(1, blocks * 1 // 2, blocks // 2)
    loads[2].wait()

    peer = lax.rem(t + 1, n_tp)
    other_rows = attended[pl.ds(pl.multiple_of(peer * half, half), half), :]
    own_rows = attended[pl.ds(pl.multiple_of(t * half, half), half), :]

    def swap_half(j):
        return remote(
            leaving.at[origin[j]], arriving.at[origin[j]], t_send.at[0], t_recv.at[j], "tp", peer
        )

    def project(j):
        weight = whole(2, j)
        leaving[origin[j]] = jnp.dot(
            other_rows, weight, preferred_element_type=jnp.float32
        ).astype(jnp.bfloat16)
        swap_half(j).start()
        kept[origin[j]] = jnp.dot(own_rows, weight, preferred_element_type=jnp.float32)

    pass_far(14)
    project(0)
    take(10)
    relay(12)
    take(9)
    project(1)
    relay(14)
    project(2)
    take(11)
    project(3)

    square = jnp.zeros((half, 1), jnp.float32)
    for j in range(n_kv):
        slot = origin[j]
        swap_half(j).wait_recv()
        mixed = kept[slot] + arriving[slot].astype(jnp.float32)
        kept[slot] = mixed
        square += jnp.sum(mixed * mixed, axis=1, keepdims=True)
    scale = lax.rsqrt(square * (1.0 / width) + 1e-06)
    for j in range(n_kv):
        columns = slice(j * depth, (j + 1) * depth)
        result[:, columns] = (kept[j] * scale * gain[:, columns]).astype(jnp.bfloat16)

    def drain(slots, sem):
        remote(slots, slots, sem, z_recv.at[0], "kv", origin[1]).wait_send()

    edge = out_all.shape[2] // PIECES[2] * (PIECES[2] - FAR)
    drain(pair_all.at[0 : n_kv - 1, 0:2], d_send.at[0])
    drain(query_all.at[0 : n_kv - 1, :, 0:2], d_send.at[1])
    drain(out_all.at[0 : n_kv - 1, 0:2], d_send.at[2])
    drain(pair_all.at[0 : n_kv - 1, 0], r_send.at[0])
    drain(query_all.at[0 : n_kv - 1, :, 0], r_send.at[1])
    if edge:
        drain(out_all.at[0 : n_kv - 1, 0, 0:edge], r_send.at[2])

    def drain_planes(planes):
        drain(pair_all.at[0:planes, 0], z_send.at[0])
        drain(query_all.at[0:planes, :, 0], z_send.at[1])
        drain(out_all.at[0:planes, 0], z_send.at[2])
        if FAR:
            drain(out_all.at[0:planes, 0, edge:], c_send.at[0])

    @pl.when(middle)
    def _():
        drain_planes(n_kv)

    @pl.when(jnp.logical_not(middle))
    def _():
        drain_planes(n_kv - 2)

    drain(packed.at[1:n_kv], kv_send.at[0])
    drain(asks.at[0 : n_kv - 1], ask_send.at[0])
    drain(leaving, t_send.at[0])


def per_device_fused(
    n_dp, n_kv, n_tp,
    tokens, chosen, query_weight, key_matrix, value_matrix, out_weight, out_gain,
):
    rows, width = tokens.shape
    depth, columns = query_weight.shape
    blocks = rows // BLOCK_LENGTH
    cut = lambda w: w.reshape(n_dp, w.shape[0] // n_dp, w.shape[1])
    query, out = cut(query_weight), cut(out_weight)
    pair = jax.ShapeDtypeStruct((n_dp, LANES, depth // n_dp), jnp.bfloat16)
    bf16, f32 = jnp.bfloat16, jnp.float32
    vmem = pl.BlockSpec(memory_space=pltpu.VMEM)
    off_core = pl.BlockSpec(memory_space=pltpu.HBM)
    dma = pltpu.SemaphoreType.DMA
    copies = sum(PIECES) * (n_kv - 1)
    return pl.pallas_call(
        functools.partial(fused, n_dp, n_kv, n_tp),
        out_shape=pltpu.VMEM((rows // n_tp, width), bf16),
        in_specs=[
            off_core, off_core, off_core, off_core, off_core, off_core, off_core,
        ],
        out_specs=vmem,
        scratch_shapes=[
            pltpu.SMEM((blocks, chosen.shape[1]), jnp.int32),
            pltpu.SMEM((blocks, chosen.shape[1]), jnp.int32),
            pltpu.SMEM((n_kv,), jnp.int32),
            pltpu.VMEM((1, width), f32),
            pltpu.VMEM((rows, width), bf16),
            pltpu.VMEM(pair.shape, bf16),
            pltpu.VMEM((PIECES[1],) + query.shape[:2] + (columns // PIECES[1],), bf16),
            pltpu.VMEM(out.shape, bf16),
            pltpu.VMEM((blocks, chosen.shape[1]), jnp.int32),
            pltpu.VMEM((n_kv, blocks, chosen.shape[1]), jnp.int32),
            pltpu.VMEM((n_kv, CAP, BLOCK_LENGTH, LANES), bf16),
            pltpu.VMEM((blocks, BLOCK_LENGTH, LANES), bf16),
            pltpu.VMEM((n_kv * CAP, BLOCK_LENGTH, LANES), bf16),
            pltpu.VMEM((n_kv,) + pair.shape, bf16),
            pltpu.VMEM(
                (n_kv, PIECES[1]) + query.shape[:2] + (columns // PIECES[1],), bf16
            ),
            pltpu.VMEM((n_kv,) + out.shape, bf16),
            pltpu.VMEM((n_kv * CAP + blocks, BLOCK_LENGTH, LANES), bf16),
            pltpu.VMEM((rows, columns // PIECES[1]), f32),
            pltpu.VMEM((columns // HEAD_WIDTH, rows, LANES), bf16),
            pltpu.VMEM((rows, columns), bf16),
            pltpu.VMEM((n_kv, rows // n_tp, width // n_kv), bf16),
            pltpu.VMEM((n_kv, rows // n_tp, width // n_kv), bf16),
            pltpu.VMEM((n_kv, rows // n_tp, width // n_kv), f32),
            dma((6 + PIECES[1],)), dma((3,)), dma((copies,)), dma((1,)), dma((max(1, FAR * (n_kv - 1)),)),
            dma((3,)), dma((copies,)), dma((3,)), dma((copies,)),
            dma((1,)), dma((1,)), dma((1,)), dma((n_kv,)), dma((1,)), dma((1,)),
        ],
        compiler_params=pltpu.CompilerParams(
            collective_id=0, has_side_effects=True, vmem_limit_bytes=54 * 1024 * 1024
        ),
    )(chosen, tokens, key_matrix.T, value_matrix.T, query, out, out_gain.reshape(1, width))


def per_device(tokens, chosen, query_weight, key_matrix, value_matrix, out_weight, out_gain):
    tok_rows = tokens.shape[0]
    blocks = tok_rows // BLOCK_LENGTH
    device = lax.axis_index("kv")
    kv_count = lax.axis_size("kv")
    whole_query, whole_key, whole_value = (
        lax.all_gather(query_weight, "kv", axis=0, tiled=True),
        lax.all_gather(key_matrix, "kv", axis=0, tiled=True),
        lax.all_gather(value_matrix, "kv", axis=0, tiled=True),
    )
    query_rows = jnp.dot(tokens, whole_query, preferred_element_type=jnp.float32).astype(
        jnp.bfloat16
    )
    key_rows = jnp.dot(tokens, whole_key, preferred_element_type=jnp.float32).astype(jnp.bfloat16)
    value_rows = jnp.dot(tokens, whole_value, preferred_element_type=jnp.float32).astype(
        jnp.bfloat16
    )
    paired = jnp.concatenate([key_rows, value_rows], axis=1)
    pair_width = paired.shape[1]
    safe_ids = jnp.maximum(chosen, 0)
    everyone = lax.all_gather(paired, "kv", axis=0, tiled=True).reshape(
        kv_count * blocks, BLOCK_LENGTH, pair_width
    )
    picked = jnp.take(everyone, safe_ids, axis=0)
    head_count = query_rows.shape[1] // HEAD_WIDTH
    grouped = query_rows.reshape(blocks, BLOCK_LENGTH, head_count, HEAD_WIDTH)
    offsets = jnp.arange(BLOCK_LENGTH, dtype=jnp.int32)
    query_pos = (device * blocks + jnp.arange(blocks, dtype=jnp.int32))[
        :, None
    ] * BLOCK_LENGTH + offsets[None, :]
    key_pos = safe_ids[:, :, None] * BLOCK_LENGTH + offsets[None, None, :]
    visible = (chosen >= 0)[:, None, :, None] & (
        key_pos[:, None, :, :] <= query_pos[:, :, None, None]
    )

    def attend_block(inputs):
        query_block, pair_block, seen = inputs
        block_keys = pair_block[..., :HEAD_WIDTH]
        block_values = pair_block[..., HEAD_WIDTH:]
        scores = jnp.einsum(
            "qgd,skd->gqsk", query_block, block_keys, preferred_element_type=jnp.float32
        ) * HEAD_WIDTH ** (-0.5)
        scores = jnp.where(seen[None], scores, -1e30)
        row_max = jnp.max(scores, axis=(2, 3), keepdims=True)
        expon = jnp.exp(scores - row_max)
        row_sum = jnp.sum(expon, axis=(2, 3), keepdims=True)
        weights_bf = (expon / row_sum).astype(jnp.bfloat16)
        result = jnp.einsum(
            "gqsk,skd->qgd", weights_bf, block_values, preferred_element_type=jnp.float32
        )
        return result.astype(jnp.bfloat16)

    attended = lax.map(attend_block, (grouped, picked, visible))
    attended = attended.reshape(tok_rows, head_count * HEAD_WIDTH)
    whole_out = lax.all_gather(out_weight, "kv", axis=1, tiled=True)
    mixed = lax.psum_scatter(
        jnp.dot(attended, whole_out, preferred_element_type=jnp.float32).astype(jnp.bfloat16),
        "tp",
        scatter_dimension=0,
        tiled=True,
    ).astype(jnp.float32)
    normed = mixed * lax.rsqrt(jnp.mean(mixed * mixed, axis=-1, keepdims=True) + 1e-06) * out_gain
    return normed.astype(jnp.bfloat16)


def solution(mesh):
    placed = (
        P(("dp", "kv"), None),
        P(("dp", "kv"), None),
        P("kv", "tp"),
        P("kv", "tp"),
        P("kv", "tp"),
        P("tp", "kv"),
        P(),
    )
    n_dp, n_kv, n_tp = (mesh.shape[name] for name in ("dp", "kv", "tp"))

    def body(tokens, chosen, query_weight, key_matrix, value_matrix, out_weight, out_gain):
        args = (tokens, chosen, query_weight, key_matrix, value_matrix, out_weight, out_gain)
        depth, columns = query_weight.shape
        whole_tiles = (
            depth % (LANES * n_dp) == 0
            and columns % (2 * LANES * PIECES[1]) == 0
            and columns % (2 * LANES * PIECES[1]) == 0
            and out_weight.shape[0] % (32 * PIECES[2] * n_dp) == 0
            and out_weight.shape[1] % LANES == 0
            and columns % LANES == 0
            and key_matrix.shape[1] == HEAD_WIDTH
            and chosen.shape[1] % 2 == 0
            and n_tp == 2
            and n_dp == 4
            and n_kv == 4
            and tokens.shape[0] == 8 * BLOCK_LENGTH
        )
        if whole_tiles:
            return per_device_fused(n_dp, n_kv, n_tp, *args)
        return per_device(*args)

    return jax.shard_map(
        body,
        mesh=mesh,
        in_specs=placed,
        out_specs=P(("dp", "kv", "tp"), None),
        check_vma=False,
    )
```

```python
import functools

import jax
import jax.numpy as jnp
from jax import lax
from jax.experimental import pallas as pl
from jax.experimental.pallas import tpu as pltpu
from jax.sharding import PartitionSpec as P

HEAD_WIDTH = 64
BLOCK_LENGTH = 64
LANES = 2 * HEAD_WIDTH
HIDDEN = -1e30
CAP = 2
PIECES = (1, 2, 2)
FAR = 1


def remote(src, dst, send, recv, axis, peer):
    return pltpu.make_async_remote_copy(
        src_ref=src,
        dst_ref=dst,
        send_sem=send,
        recv_sem=recv,
        device_id={axis: peer},
        device_id_type=pl.DeviceIdType.MESH,
    )


def fused(
    n_dp, n_kv, n_tp,
    chosen_hbm, tokens_hbm, key_hbm, value_hbm, query_hbm, out_hbm, gain_hbm, result,
    chosen, spots, lowest_of, picked, gain, tokens, pair_own, query_own, out_own, wanted, asks, packed, kv_own, kv_far,
    pair_all, query_all, out_all, keys, values, query_sum, query_rows, attended,
    leaving, arriving, kept,
    load_sem, z_send, z_recv, c_send, c_recv, d_send, d_recv, r_send, r_recv, kv_send, kv_recv, t_send, t_recv, ask_send, ask_recv,
):
    d, z, t = lax.axis_index("dp"), lax.axis_index("kv"), lax.axis_index("tp")
    rows, width = tokens.shape
    blocks = rows // BLOCK_LENGTH
    depth = width // n_kv
    half = rows // n_tp
    cut = depth // n_dp
    loads = [
        pltpu.make_async_copy(source, target, load_sem.at[k])
        for k, (source, target) in enumerate(
            ((tokens_hbm, tokens), (out_hbm, out_own), (gain_hbm, gain), (chosen_hbm, wanted),
             (chosen_hbm, chosen))
        )
    ]
    part_width = query_own.shape[3]
    query_loads = [
        pltpu.make_async_copy(
            query_hbm.at[:, :, part * part_width : (part + 1) * part_width], query_own.at[part],
            load_sem.at[6 + part],
        )
        for part in range(PIECES[1])
    ]
    pair_loads = [
        pltpu.make_async_copy(
            source.at[:, k * cut : (k + 1) * cut],
            pair_own.at[k, side * HEAD_WIDTH : (side + 1) * HEAD_WIDTH],
            load_sem.at[5],
        )
        for k in range(n_dp)
        for side, source in enumerate((key_hbm, value_hbm))
    ]
    for load in pair_loads + loads[3:4] + query_loads + loads[:3] + loads[4:]:
        load.start()

    barrier = pltpu.get_barrier_semaphore()
    for axis, me, count in (("dp", d, n_dp), ("kv", z, n_kv), ("tp", t, n_tp)):
        for step in range(1, count):
            pl.semaphore_signal(
                barrier, inc=1, device_id={axis: lax.rem(me + step, count)},
                device_id_type=pl.DeviceIdType.MESH,
            )
    pl.semaphore_wait(barrier, n_dp + n_kv + n_tp - 3)

    owns = (pair_own, query_own, out_own)
    alls = (pair_all, query_all, out_all)
    events = [
        (which, part, j) for which in range(3) for part in range(PIECES[which]) for j in range(1, n_kv)
    ]
    far = [e for e, event in enumerate(events) if event[0] == 2 and event[1] >= PIECES[2] - FAR]
    origin = (z, z + 1 - 2 * lax.rem(z, 2), lax.rem(z + 2, 4), 3 - z)
    middle = (z == 1) | (z == 2)
    near = (d, d + 1 - 2 * lax.rem(d, 2), lax.rem(d + 2, 4))
    corner = 3 - d

    def piece_of(e, planes, plane, quarter, share=0, shares=1):
        which, part, _ = events[e]
        lead = (plane,) if planes else ()
        refs = alls if planes else owns
        if which == 1:
            size = refs[which].shape[-2] // shares
            return refs[which].at[(*lead, part, quarter, pl.ds(share * size, size))]
        size = refs[which].shape[-2] // PIECES[which]
        span = pl.ds(part * size + share * (size // shares), size // shares)
        return refs[which].at[(*lead, quarter, span)]

    def slot(e, quarter, share=0, shares=1):
        return piece_of(e, True, origin[events[e][2]], quarter, share, shares)

    def across(e, quarter, send, recv):
        return remote(
            piece_of(e, False, None, quarter), piece_of(e, True, z, quarter), send, recv,
            "kv", origin[events[e][2]],
        )

    def first(e):
        return across(e, d, z_send.at[events[e][0]], z_recv.at[e])

    def first_far(e):
        return across(e, corner, c_send.at[0], c_recv.at[far.index(e)])

    def landed(e, quarter, recv):
        place = slot(e, quarter)
        return remote(place, place, c_send.at[0], recv, "kv", origin[1])

    def onward(e):
        place = slot(e, d)
        return remote(place, place, z_send.at[events[e][0]], z_recv.at[e + 1], "kv", origin[1])

    def onward_far(e):
        place = slot(e, corner)
        return remote(
            place, place, c_send.at[0], c_recv.at[far.index(e) + 1], "kv", origin[1]
        )

    def second(e, k):
        place = slot(e, d)
        return remote(place, place, d_send.at[events[e][0]], d_recv.at[e], "dp", near[k])

    def second_in(e):
        places = slot(e, pl.ds(0, 2))
        return remote(places, places, d_send.at[events[e][0]], d_recv.at[e], "dp", near[1])

    def halfway(e, k):
        place = slot(e, near[k], k - 1, 2)
        return remote(place, place, r_send.at[events[e][0]], r_recv.at[e], "dp", near[3 - k])

    def halfway_in(e):
        place = slot(e, corner)
        return remote(place, place, r_send.at[events[e][0]], r_recv.at[e], "dp", near[1])

    def begin(copy, e):
        if events[e][2] == 3:

            @pl.when(middle)
            def _():
                copy(e).start()
        else:
            copy(e).start()

    def hand_on(copy, e):
        if events[e][2] == 2:

            @pl.when(middle)
            def _():
                copy(e).start()

    def out(e):
        begin(first, e)

    def out_far(e):
        begin(first_far, e)

    def pass_on(e):
        landed(e, d, z_recv.at[e]).wait_recv()
        hand_on(onward, e)
        for k in (1, 2):
            second(e, k).start()

    def pass_far(e):
        landed(e, corner, c_recv.at[far.index(e)]).wait_recv()
        hand_on(onward_far, e)

    def relay(e):
        second_in(e).wait_recv()
        if e not in far:
            for k in (1, 2):
                halfway(e, k).start()

    def take(e):
        halfway_in(e).wait_recv()

    def whole(which, j, part=None):
        block = owns[which] if j == 0 else alls[which].at[origin[j]]
        block = block[...] if part is None else block[part]
        return block.reshape(block.shape[0] * block.shape[1], block.shape[2])

    def token_part(j):
        start = pl.multiple_of(origin[j] * depth, depth)
        return tokens[:, pl.ds(start, depth)]

    def ask(j):
        return remote(wanted, asks.at[z], ask_send.at[0], ask_recv.at[0], "kv", origin[j])

    def asks_in():
        slots = asks.at[0 : n_kv - 1]
        return remote(slots, slots, ask_send.at[0], ask_recv.at[0], "kv", origin[1])

    def pair_part(j):
        block = pair_own[...] if j == 0 else pair_all[origin[j]]
        block = jnp.concatenate([block[k] for k in range(n_dp)], axis=1)
        return lax.dot_general(
            token_part(j), block, (((1,), (1,)), ((), ())), preferred_element_type=jnp.float32
        )

    def pair_stage():
        total = pair_part(0)
        for j in range(1, n_kv):
            total += pair_part(j)
        kv_own[...] = total.astype(jnp.bfloat16).reshape(blocks, BLOCK_LENGTH, LANES)

    def named(rows_of, owner):
        local = rows_of - owner * blocks
        inside = (local >= 0) & (local < blocks)
        return (
            jnp.min(jnp.where(inside, local, blocks - 1)),
            jnp.max(jnp.where(inside, local, 0)),
        )

    def kv_out(j):
        return remote(
            packed.at[j], kv_far.at[pl.ds(z * CAP, CAP)], kv_send.at[0], kv_recv.at[0],
            "kv", origin[j],
        )

    def kv_in(count):
        slots = kv_far.at[0 : count * CAP]
        return remote(slots, slots, kv_send.at[0], kv_recv.at[0], "kv", origin[1])

    later_peer = (None, lax.rem(z, 2) == 0, z < 2, z < 2)

    picks = chosen.shape[1]

    absent = n_kv * CAP + blocks

    def locate(b, carry):
        for s in range(picks):
            name = jnp.maximum(chosen[b, s], 0)
            owner = lax.div(name, blocks)
            far = owner * CAP + jnp.where(name == lowest_of[owner], 0, 1)
            here = jnp.where(owner == z, name - z * blocks + n_kv * CAP, far)
            spots[b, s] = jnp.where(chosen[b, s] >= 0, here, absent)
        return carry

    def plan_blocks():
        for owner in range(n_kv):

            @pl.when(z <= owner)
            def _(owner=owner):
                kv_far[owner * CAP : (owner + 1) * CAP] = jnp.zeros(
                    (CAP, BLOCK_LENGTH, LANES), jnp.bfloat16
                )

        for owner in range(n_kv):
            lowest_of[owner] = named(wanted[...], owner)[0] + owner * blocks
        lax.fori_loop(0, blocks, locate, 0)
        asks_in().wait_recv()
        for j in range(1, n_kv):
            picked[j, 0], picked[j, 1] = named(asks[origin[j]], z)

    def share_blocks():
        for j in range(1, n_kv):
            for side in range(2):
                packed[j, side] = kv_own[picked[j, side]]

            @pl.when(later_peer[j])
            def _(j=j):
                kv_out(j).start()

    def query_part(part, j):
        term = jnp.dot(
            token_part(j), whole(1, j, part), preferred_element_type=jnp.float32
        )
        query_sum[...] = term if j == 0 else query_sum[...] + term

    heads = query_rows.shape[0]
    group = heads // PIECES[1]

    def query_tiles(part):
        spread = lax.broadcasted_iota(jnp.int32, (rows, LANES), 1)
        at_head = spread < HEAD_WIDTH
        flag = jnp.where(spread == HEAD_WIDTH, 1.0, 0.0)
        for p in range(group // 2):
            both = query_sum[:, p * LANES : (p + 1) * LANES]
            for side, one in enumerate((both, pltpu.roll(both, HEAD_WIDTH, 1))):
                one = one.astype(jnp.bfloat16) * jnp.bfloat16(HEAD_WIDTH ** (-0.5))
                query_rows[part * group + 2 * p + side] = jnp.where(
                    at_head, one.astype(jnp.float32), flag
                ).astype(jnp.bfloat16)

    lane = lax.broadcasted_iota(jnp.int32, (BLOCK_LENGTH, LANES), 1)
    row = lax.broadcasted_iota(jnp.int32, (BLOCK_LENGTH, LANES), 0)
    low = lane < HEAD_WIDTH
    later_keys = jnp.where(low & (lane > row), HIDDEN, 0.0)

    def gather_blocks():
        for count in range(1, n_kv):

            @pl.when(z == count)
            def _(count=count):
                kv_in(count).wait_recv()

        for source, start in ((kv_far, 0), (kv_own, n_kv * CAP)):
            both = source[...].astype(jnp.float32)
            left = lax.broadcasted_iota(jnp.int32, both.shape, 2) < HEAD_WIDTH
            keys[start : start + both.shape[0]] = jnp.where(left, both, 0.0).astype(jnp.bfloat16)
            values[start : start + both.shape[0]] = jnp.where(left, 1.0, both).astype(jnp.bfloat16)
        keys[absent] = jnp.where(lane == HEAD_WIDTH, HIDDEN, 0.0).astype(jnp.bfloat16)
        values[absent] = jnp.zeros((BLOCK_LENGTH, LANES), jnp.bfloat16)

    def chosen_rows(source, b):
        return jnp.concatenate([source[spots[b, s]] for s in range(picks)], axis=0)

    def score(part, b):
        query = query_rows[
            part * group : (part + 1) * group, b * BLOCK_LENGTH : (b + 1) * BLOCK_LENGTH, :
        ].reshape(group * BLOCK_LENGTH, LANES)
        return lax.dot_general(
            query, chosen_rows(keys, b), (((1,), (1,)), ((), ())),
            preferred_element_type=jnp.float32,
        )

    ahead = []

    def attend(part, start, count):
        for b in range(start, start + count):
            scores = ahead.pop() if ahead else score(part, b)
            if b + 1 < blocks:
                ahead.append(score(part, b + 1))
            scores = scores.reshape(group, BLOCK_LENGTH, picks * BLOCK_LENGTH)
            head, rest = scores[:, :, :LANES] + later_keys[None], scores[:, :, LANES:]
            top = jnp.maximum(
                jnp.max(head, axis=2, keepdims=True), jnp.max(rest, axis=2, keepdims=True)
            )
            expon = jnp.concatenate([jnp.exp(head - top), jnp.exp(rest - top)], axis=2)
            probs = expon.astype(jnp.bfloat16).reshape(group * BLOCK_LENGTH, picks * BLOCK_LENGTH)
            mixed = jnp.dot(probs, chosen_rows(values, b), preferred_element_type=jnp.float32)
            mixed = mixed.reshape(group, BLOCK_LENGTH, LANES)
            for p in range(group // 2):
                even, odd = mixed[2 * p], mixed[2 * p + 1]
                joined = jnp.where(
                    low,
                    pltpu.roll(even, HEAD_WIDTH, 1) / even,
                    odd / pltpu.roll(odd, HEAD_WIDTH, 1),
                )
                column = (part * group // 2 + p) * LANES
                attended[b * BLOCK_LENGTH : (b + 1) * BLOCK_LENGTH, column : column + LANES] = (
                    joined.astype(jnp.bfloat16)
                )

    loads[3].wait()
    for j in range(1, n_kv):
        ask(j).start()
    pltpu.make_async_copy(pair_own, pair_own, load_sem.at[5]).wait()
    out(1)
    query_loads[1].wait()
    for e in (6, 2, 0):
        out(e)
    query_loads[0].wait()
    for e in (4, 5):
        out(e)
    for e in (1, 6, 0):
        pass_on(e)
    out(3)
    loads[4].wait()
    plan_blocks()
    pass_on(2)
    out(7)
    pass_on(4)
    relay(0)
    pass_on(3)
    relay(1)
    loads[1].wait()
    for e in (10, 12, 8):
        out(e)
    relay(2)
    out(13)
    for e in (5, 7):
        pass_on(e)
    take(1)
    relay(3)
    take(0)
    relay(4)
    take(2)
    loads[0].wait()
    pair_stage()
    share_blocks()
    for e in (5, 6):
        relay(e)
    pass_on(8)
    out(9)
    pass_on(10)
    query_part(0, 0)
    take(3)
    relay(7)
    out(11)
    take(4)
    query_part(0, 1)
    take(5)
    query_part(0, 2)
    query_part(0, 3)
    out_far(12)
    out(14)
    query_tiles(0)
    out_far(13)
    gather_blocks()
    pass_on(9)
    attend(0, blocks * 0 // 2, blocks // 2)
    relay(8)
    pass_on(13)
    take(6)
    query_part(1, 0)
    query_part(1, 1)
    take(7)
    attend(0, blocks * 1 // 2, blocks // 2)
    pass_on(11)
    out_far(14)
    relay(10)
    query_part(1, 2)
    take(8)
    pass_on(12)
    query_part(1, 3)
    pass_on(14)
    query_tiles(1)
    relay(9)
    pass_far(13)
    attend(1, blocks * 0 // 2, blocks // 2)
    relay(11)
    attend(1, blocks * 1 // 2, blocks // 2)
    loads[2].wait()

    peer = lax.rem(t + 1, n_tp)
    other_rows = attended[pl.ds(pl.multiple_of(peer * half, half), half), :]
    own_rows = attended[pl.ds(pl.multiple_of(t * half, half), half), :]

    def swap_half(j):
        return remote(
            leaving.at[origin[j]], arriving.at[origin[j]], t_send.at[0], t_recv.at[j], "tp", peer
        )

    def project(j):
        weight = whole(2, j)
        leaving[origin[j]] = jnp.dot(
            other_rows, weight, preferred_element_type=jnp.float32
        ).astype(jnp.bfloat16)
        swap_half(j).start()
        kept[origin[j]] = jnp.dot(own_rows, weight, preferred_element_type=jnp.float32)

    relay(13)
    for e in (12, 14):
        pass_far(e)
    project(0)
    take(10)
    relay(12)
    take(9)
    project(1)
    relay(14)
    project(2)
    take(11)
    project(3)

    square = jnp.zeros((half, 1), jnp.float32)
    for j in range(n_kv):
        slot = origin[j]
        swap_half(j).wait_recv()
        mixed = kept[slot] + arriving[slot].astype(jnp.float32)
        kept[slot] = mixed
        square += jnp.sum(mixed * mixed, axis=1, keepdims=True)
    scale = lax.rsqrt(square * (1.0 / width) + 1e-06)
    for j in range(n_kv):
        columns = slice(j * depth, (j + 1) * depth)
        result[:, columns] = (kept[j] * scale * gain[:, columns]).astype(jnp.bfloat16)

    def drain(slots, sem):
        remote(slots, slots, sem, z_recv.at[0], "kv", origin[1]).wait_send()

    edge = out_all.shape[2] // PIECES[2] * (PIECES[2] - FAR)
    drain(pair_all.at[0 : n_kv - 1, 0:2], d_send.at[0])
    drain(query_all.at[0 : n_kv - 1, :, 0:2], d_send.at[1])
    drain(out_all.at[0 : n_kv - 1, 0:2], d_send.at[2])
    drain(pair_all.at[0 : n_kv - 1, 0], r_send.at[0])
    drain(query_all.at[0 : n_kv - 1, :, 0], r_send.at[1])
    if edge:
        drain(out_all.at[0 : n_kv - 1, 0, 0:edge], r_send.at[2])

    def drain_planes(planes):
        drain(pair_all.at[0:planes, 0], z_send.at[0])
        drain(query_all.at[0:planes, :, 0], z_send.at[1])
        drain(out_all.at[0:planes, 0], z_send.at[2])
        if FAR:
            drain(out_all.at[0:planes, 0, edge:], c_send.at[0])

    @pl.when(middle)
    def _():
        drain_planes(n_kv)

    @pl.when(jnp.logical_not(middle))
    def _():
        drain_planes(n_kv - 2)

    for count in range(1, n_kv):

        @pl.when(z == n_kv - 1 - count)
        def _(count=count):
            drain(packed.at[1 : count + 1], kv_send.at[0])

    drain(asks.at[0 : n_kv - 1], ask_send.at[0])
    drain(leaving, t_send.at[0])


def per_device_fused(
    n_dp, n_kv, n_tp,
    tokens, chosen, query_weight, key_matrix, value_matrix, out_weight, out_gain,
):
    rows, width = tokens.shape
    depth, columns = query_weight.shape
    blocks = rows // BLOCK_LENGTH
    cut = lambda w: w.reshape(n_dp, w.shape[0] // n_dp, w.shape[1])
    query, out = cut(query_weight), cut(out_weight)
    pair = jax.ShapeDtypeStruct((n_dp, LANES, depth // n_dp), jnp.bfloat16)
    bf16, f32 = jnp.bfloat16, jnp.float32
    vmem = pl.BlockSpec(memory_space=pltpu.VMEM)
    off_core = pl.BlockSpec(memory_space=pltpu.HBM)
    dma = pltpu.SemaphoreType.DMA
    copies = sum(PIECES) * (n_kv - 1)
    return pl.pallas_call(
        functools.partial(fused, n_dp, n_kv, n_tp),
        out_shape=pltpu.VMEM((rows // n_tp, width), bf16),
        in_specs=[
            off_core, off_core, off_core, off_core, off_core, off_core, off_core,
        ],
        out_specs=vmem,
        scratch_shapes=[
            pltpu.SMEM((blocks, chosen.shape[1]), jnp.int32),
            pltpu.SMEM((blocks, chosen.shape[1]), jnp.int32),
            pltpu.SMEM((n_kv,), jnp.int32),
            pltpu.SMEM((n_kv, 2), jnp.int32),
            pltpu.VMEM((1, width), f32),
            pltpu.VMEM((rows, width), bf16),
            pltpu.VMEM(pair.shape, bf16),
            pltpu.VMEM((PIECES[1],) + query.shape[:2] + (columns // PIECES[1],), bf16),
            pltpu.VMEM(out.shape, bf16),
            pltpu.VMEM((blocks, chosen.shape[1]), jnp.int32),
            pltpu.VMEM((n_kv, blocks, chosen.shape[1]), jnp.int32),
            pltpu.VMEM((n_kv, CAP, BLOCK_LENGTH, LANES), bf16),
            pltpu.VMEM((blocks, BLOCK_LENGTH, LANES), bf16),
            pltpu.VMEM((n_kv * CAP, BLOCK_LENGTH, LANES), bf16),
            pltpu.VMEM((n_kv,) + pair.shape, bf16),
            pltpu.VMEM(
                (n_kv, PIECES[1]) + query.shape[:2] + (columns // PIECES[1],), bf16
            ),
            pltpu.VMEM((n_kv,) + out.shape, bf16),
            pltpu.VMEM((n_kv * CAP + blocks + 1, BLOCK_LENGTH, LANES), bf16),
            pltpu.VMEM((n_kv * CAP + blocks + 1, BLOCK_LENGTH, LANES), bf16),
            pltpu.VMEM((rows, columns // PIECES[1]), f32),
            pltpu.VMEM((columns // HEAD_WIDTH, rows, LANES), bf16),
            pltpu.VMEM((rows, columns), bf16),
            pltpu.VMEM((n_kv, rows // n_tp, width // n_kv), bf16),
            pltpu.VMEM((n_kv, rows // n_tp, width // n_kv), bf16),
            pltpu.VMEM((n_kv, rows // n_tp, width // n_kv), f32),
            dma((6 + PIECES[1],)), dma((3,)), dma((copies,)), dma((1,)), dma((max(1, FAR * (n_kv - 1)),)),
            dma((3,)), dma((copies,)), dma((3,)), dma((copies,)),
            dma((1,)), dma((1,)), dma((1,)), dma((n_kv,)), dma((1,)), dma((1,)),
        ],
        compiler_params=pltpu.CompilerParams(
            collective_id=0, has_side_effects=True, vmem_limit_bytes=54 * 1024 * 1024
        ),
    )(chosen, tokens, key_matrix.T, value_matrix.T, query, out, out_gain.reshape(1, width))


def per_device(tokens, chosen, query_weight, key_matrix, value_matrix, out_weight, out_gain):
    tok_rows = tokens.shape[0]
    blocks = tok_rows // BLOCK_LENGTH
    device = lax.axis_index("kv")
    kv_count = lax.axis_size("kv")
    whole_query, whole_key, whole_value = (
        lax.all_gather(query_weight, "kv", axis=0, tiled=True),
        lax.all_gather(key_matrix, "kv", axis=0, tiled=True),
        lax.all_gather(value_matrix, "kv", axis=0, tiled=True),
    )
    query_rows = jnp.dot(tokens, whole_query, preferred_element_type=jnp.float32).astype(
        jnp.bfloat16
    )
    key_rows = jnp.dot(tokens, whole_key, preferred_element_type=jnp.float32).astype(jnp.bfloat16)
    value_rows = jnp.dot(tokens, whole_value, preferred_element_type=jnp.float32).astype(
        jnp.bfloat16
    )
    paired = jnp.concatenate([key_rows, value_rows], axis=1)
    pair_width = paired.shape[1]
    safe_ids = jnp.maximum(chosen, 0)
    everyone = lax.all_gather(paired, "kv", axis=0, tiled=True).reshape(
        kv_count * blocks, BLOCK_LENGTH, pair_width
    )
    picked = jnp.take(everyone, safe_ids, axis=0)
    head_count = query_rows.shape[1] // HEAD_WIDTH
    grouped = query_rows.reshape(blocks, BLOCK_LENGTH, head_count, HEAD_WIDTH)
    offsets = jnp.arange(BLOCK_LENGTH, dtype=jnp.int32)
    query_pos = (device * blocks + jnp.arange(blocks, dtype=jnp.int32))[
        :, None
    ] * BLOCK_LENGTH + offsets[None, :]
    key_pos = safe_ids[:, :, None] * BLOCK_LENGTH + offsets[None, None, :]
    visible = (chosen >= 0)[:, None, :, None] & (
        key_pos[:, None, :, :] <= query_pos[:, :, None, None]
    )

    def attend_block(inputs):
        query_block, pair_block, seen = inputs
        block_keys = pair_block[..., :HEAD_WIDTH]
        block_values = pair_block[..., HEAD_WIDTH:]
        scores = jnp.einsum(
            "qgd,skd->gqsk", query_block, block_keys, preferred_element_type=jnp.float32
        ) * HEAD_WIDTH ** (-0.5)
        scores = jnp.where(seen[None], scores, -1e30)
        row_max = jnp.max(scores, axis=(2, 3), keepdims=True)
        expon = jnp.exp(scores - row_max)
        row_sum = jnp.sum(expon, axis=(2, 3), keepdims=True)
        weights_bf = (expon / row_sum).astype(jnp.bfloat16)
        result = jnp.einsum(
            "gqsk,skd->qgd", weights_bf, block_values, preferred_element_type=jnp.float32
        )
        return result.astype(jnp.bfloat16)

    attended = lax.map(attend_block, (grouped, picked, visible))
    attended = attended.reshape(tok_rows, head_count * HEAD_WIDTH)
    whole_out = lax.all_gather(out_weight, "kv", axis=1, tiled=True)
    mixed = lax.psum_scatter(
        jnp.dot(attended, whole_out, preferred_element_type=jnp.float32).astype(jnp.bfloat16),
        "tp",
        scatter_dimension=0,
        tiled=True,
    ).astype(jnp.float32)
    normed = mixed * lax.rsqrt(jnp.mean(mixed * mixed, axis=-1, keepdims=True) + 1e-06) * out_gain
    return normed.astype(jnp.bfloat16)


def solution(mesh):
    placed = (
        P(("dp", "kv"), None),
        P(("dp", "kv"), None),
        P("kv", "tp"),
        P("kv", "tp"),
        P("kv", "tp"),
        P("tp", "kv"),
        P(),
    )
    n_dp, n_kv, n_tp = (mesh.shape[name] for name in ("dp", "kv", "tp"))

    def body(tokens, chosen, query_weight, key_matrix, value_matrix, out_weight, out_gain):
        args = (tokens, chosen, query_weight, key_matrix, value_matrix, out_weight, out_gain)
        depth, columns = query_weight.shape
        whole_tiles = (
            depth % (LANES * n_dp) == 0
            and columns % (2 * LANES * PIECES[1]) == 0
            and columns % (2 * LANES * PIECES[1]) == 0
            and out_weight.shape[0] % (32 * PIECES[2] * n_dp) == 0
            and out_weight.shape[1] % LANES == 0
            and columns % LANES == 0
            and key_matrix.shape[1] == HEAD_WIDTH
            and chosen.shape[1] % 2 == 0
            and n_tp == 2
            and n_dp == 4
            and n_kv == 4
            and tokens.shape[0] == 8 * BLOCK_LENGTH
        )
        if whole_tiles:
            return per_device_fused(n_dp, n_kv, n_tp, *args)
        return per_device(*args)

    return jax.shard_map(
        body,
        mesh=mesh,
        in_specs=placed,
        out_specs=P(("dp", "kv", "tp"), None),
        check_vma=False,
    )
```

```python
import functools

import jax
import jax.numpy as jnp
from jax import lax
from jax.experimental import pallas as pl
from jax.experimental.pallas import tpu as pltpu
from jax.sharding import PartitionSpec as P

HEAD_WIDTH = 64
BLOCK_LENGTH = 64
LANES = 2 * HEAD_WIDTH
HIDDEN = -1e30
CAP = 2
PIECES = (1, 2, 2)
FAR = 1


def remote(src, dst, send, recv, axis, peer):
    return pltpu.make_async_remote_copy(
        src_ref=src,
        dst_ref=dst,
        send_sem=send,
        recv_sem=recv,
        device_id={axis: peer},
        device_id_type=pl.DeviceIdType.MESH,
    )


def fused(
    n_dp, n_kv, n_tp,
    chosen_hbm, tokens_hbm, key_hbm, value_hbm, query_hbm, out_hbm, gain_hbm, result,
    chosen, spots, lowest_of, picked, gain, tokens, pair_own, query_own, out_own, wanted, asks, packed, kv_own, kv_far,
    pair_all, query_all, out_all, keys, values, query_sum, query_rows, attended,
    leaving, arriving, kept,
    load_sem, z_send, z_recv, c_send, c_recv, d_send, d_recv, r_send, r_recv, kv_send, kv_recv, t_send, t_recv, ask_send, ask_recv,
):
    d, z, t = lax.axis_index("dp"), lax.axis_index("kv"), lax.axis_index("tp")
    rows, width = tokens.shape
    blocks = rows // BLOCK_LENGTH
    depth = width // n_kv
    half = rows // n_tp
    cut = depth // n_dp
    loads = [
        pltpu.make_async_copy(source, target, load_sem.at[k])
        for k, (source, target) in enumerate(
            ((tokens_hbm, tokens), (out_hbm, out_own), (gain_hbm, gain), (chosen_hbm, wanted),
             (chosen_hbm, chosen))
        )
    ]
    part_width = query_own.shape[3]
    query_loads = [
        pltpu.make_async_copy(
            query_hbm.at[:, :, part * part_width : (part + 1) * part_width], query_own.at[part],
            load_sem.at[6 + part],
        )
        for part in range(PIECES[1])
    ]
    pair_loads = [
        pltpu.make_async_copy(
            source.at[:, k * cut : (k + 1) * cut],
            pair_own.at[k, side * HEAD_WIDTH : (side + 1) * HEAD_WIDTH],
            load_sem.at[5],
        )
        for k in range(n_dp)
        for side, source in enumerate((key_hbm, value_hbm))
    ]
    for load in pair_loads + loads[3:4] + query_loads + loads[:3] + loads[4:]:
        load.start()

    barrier = pltpu.get_barrier_semaphore()
    partners = [("kv", lax.rem(z + step, n_kv)) for step in range(1, n_kv)]
    partners += [("dp", d + 1 - 2 * lax.rem(d, 2)), ("dp", lax.rem(d + 2, 4)), ("tp", 1 - t)]
    for axis, partner in partners:
        pl.semaphore_signal(
            barrier, inc=1, device_id={axis: partner}, device_id_type=pl.DeviceIdType.MESH
        )
    pl.semaphore_wait(barrier, len(partners))

    owns = (pair_own, query_own, out_own)
    alls = (pair_all, query_all, out_all)
    events = [
        (which, part, j) for which in range(3) for part in range(PIECES[which]) for j in range(1, n_kv)
    ]
    far = [e for e, event in enumerate(events) if event[0] == 2 and event[1] >= PIECES[2] - FAR]
    origin = (z, z + 1 - 2 * lax.rem(z, 2), lax.rem(z + 2, 4), 3 - z)
    middle = (z == 1) | (z == 2)
    near = (d, d + 1 - 2 * lax.rem(d, 2), lax.rem(d + 2, 4))
    corner = 3 - d

    def piece_of(e, planes, plane, quarter, share=0, shares=1):
        which, part, _ = events[e]
        lead = (plane,) if planes else ()
        refs = alls if planes else owns
        if which == 1:
            size = refs[which].shape[-2] // shares
            return refs[which].at[(*lead, part, quarter, pl.ds(share * size, size))]
        size = refs[which].shape[-2] // PIECES[which]
        span = pl.ds(part * size + share * (size // shares), size // shares)
        return refs[which].at[(*lead, quarter, span)]

    def slot(e, quarter, share=0, shares=1):
        return piece_of(e, True, origin[events[e][2]], quarter, share, shares)

    def across(e, quarter, send, recv):
        return remote(
            piece_of(e, False, None, quarter), piece_of(e, True, z, quarter), send, recv,
            "kv", origin[events[e][2]],
        )

    def first(e):
        return across(e, d, z_send.at[events[e][0]], z_recv.at[e])

    def first_far(e):
        return across(e, corner, c_send.at[0], c_recv.at[far.index(e)])

    def landed(e, quarter, recv):
        place = slot(e, quarter)
        return remote(place, place, c_send.at[0], recv, "kv", origin[1])

    def onward(e):
        place = slot(e, d)
        return remote(place, place, z_send.at[events[e][0]], z_recv.at[e + 1], "kv", origin[1])

    def onward_far(e):
        place = slot(e, corner)
        return remote(
            place, place, c_send.at[0], c_recv.at[far.index(e) + 1], "kv", origin[1]
        )

    def second(e, k):
        place = slot(e, d)
        return remote(place, place, d_send.at[events[e][0]], d_recv.at[e], "dp", near[k])

    def second_in(e):
        places = slot(e, pl.ds(0, 2))
        return remote(places, places, d_send.at[events[e][0]], d_recv.at[e], "dp", near[1])

    def halfway(e, k):
        place = slot(e, near[k], k - 1, 2)
        return remote(place, place, r_send.at[events[e][0]], r_recv.at[e], "dp", near[3 - k])

    def halfway_in(e):
        place = slot(e, corner)
        return remote(place, place, r_send.at[events[e][0]], r_recv.at[e], "dp", near[1])

    def begin(copy, e):
        if events[e][2] == 3:

            @pl.when(middle)
            def _():
                copy(e).start()
        else:
            copy(e).start()

    def hand_on(copy, e):
        if events[e][2] == 2:

            @pl.when(middle)
            def _():
                copy(e).start()

    def out(e):
        begin(first, e)

    def out_far(e):
        begin(first_far, e)

    def pass_on(e):
        landed(e, d, z_recv.at[e]).wait_recv()
        hand_on(onward, e)
        for k in (1, 2):
            second(e, k).start()

    def pass_far(e):
        landed(e, corner, c_recv.at[far.index(e)]).wait_recv()
        hand_on(onward_far, e)

    def relay(e):
        second_in(e).wait_recv()
        if e not in far:
            for k in (1, 2):
                halfway(e, k).start()

    def take(e):
        halfway_in(e).wait_recv()

    def whole(which, j, part=None):
        block = owns[which] if j == 0 else alls[which].at[origin[j]]
        block = block[...] if part is None else block[part]
        return block.reshape(block.shape[0] * block.shape[1], block.shape[2])

    def token_part(j):
        start = pl.multiple_of(origin[j] * depth, depth)
        return tokens[:, pl.ds(start, depth)]

    def ask(j):
        return remote(wanted, asks.at[z], ask_send.at[0], ask_recv.at[0], "kv", origin[j])

    def asks_in():
        slots = asks.at[0 : n_kv - 1]
        return remote(slots, slots, ask_send.at[0], ask_recv.at[0], "kv", origin[1])

    def pair_part(j):
        block = pair_own[...] if j == 0 else pair_all[origin[j]]
        block = jnp.concatenate([block[k] for k in range(n_dp)], axis=1)
        return lax.dot_general(
            token_part(j), block, (((1,), (1,)), ((), ())), preferred_element_type=jnp.float32
        )

    def pair_stage():
        total = pair_part(0)
        for j in range(1, n_kv):
            total += pair_part(j)
        kv_own[...] = total.astype(jnp.bfloat16).reshape(blocks, BLOCK_LENGTH, LANES)

    def named(rows_of, owner):
        local = rows_of - owner * blocks
        inside = (local >= 0) & (local < blocks)
        return (
            jnp.min(jnp.where(inside, local, blocks - 1)),
            jnp.max(jnp.where(inside, local, 0)),
        )

    def kv_out(j):
        return remote(
            packed.at[j], kv_far.at[pl.ds(z * CAP, CAP)], kv_send.at[0], kv_recv.at[0],
            "kv", origin[j],
        )

    def kv_in(count):
        slots = kv_far.at[0 : count * CAP]
        return remote(slots, slots, kv_send.at[0], kv_recv.at[0], "kv", origin[1])

    later_peer = (None, lax.rem(z, 2) == 0, z < 2, z < 2)

    picks = chosen.shape[1]

    absent = n_kv * CAP + blocks

    def locate(b, carry):
        for s in range(picks):
            name = jnp.maximum(chosen[b, s], 0)
            owner = lax.div(name, blocks)
            far = owner * CAP + jnp.where(name == lowest_of[owner], 0, 1)
            here = jnp.where(owner == z, name - z * blocks + n_kv * CAP, far)
            spots[b, s] = jnp.where(chosen[b, s] >= 0, here, absent)
        return carry

    def plan_blocks():
        for owner in range(n_kv):

            @pl.when(z <= owner)
            def _(owner=owner):
                kv_far[owner * CAP : (owner + 1) * CAP] = jnp.zeros(
                    (CAP, BLOCK_LENGTH, LANES), jnp.bfloat16
                )

        for owner in range(n_kv):
            lowest_of[owner] = named(wanted[...], owner)[0] + owner * blocks
        lax.fori_loop(0, blocks, locate, 0)
        asks_in().wait_recv()
        for j in range(1, n_kv):
            picked[j, 0], picked[j, 1] = named(asks[origin[j]], z)

    def share_blocks():
        for j in range(1, n_kv):
            for side in range(2):
                packed[j, side] = kv_own[picked[j, side]]

            @pl.when(later_peer[j])
            def _(j=j):
                kv_out(j).start()

    def query_part(part, j):
        term = jnp.dot(
            token_part(j), whole(1, j, part), preferred_element_type=jnp.float32
        )
        query_sum[...] = term if j == 0 else query_sum[...] + term

    heads = query_rows.shape[0]
    group = heads // PIECES[1]

    def query_tiles(part):
        spread = lax.broadcasted_iota(jnp.int32, (rows, LANES), 1)
        at_head = spread < HEAD_WIDTH
        flag = jnp.where(spread == HEAD_WIDTH, 1.0, 0.0)
        for p in range(group // 2):
            both = query_sum[:, p * LANES : (p + 1) * LANES]
            for side, one in enumerate((both, pltpu.roll(both, HEAD_WIDTH, 1))):
                one = one.astype(jnp.bfloat16) * jnp.bfloat16(HEAD_WIDTH ** (-0.5))
                query_rows[part * group + 2 * p + side] = jnp.where(
                    at_head, one.astype(jnp.float32), flag
                ).astype(jnp.bfloat16)

    lane = lax.broadcasted_iota(jnp.int32, (BLOCK_LENGTH, LANES), 1)
    row = lax.broadcasted_iota(jnp.int32, (BLOCK_LENGTH, LANES), 0)
    low = lane < HEAD_WIDTH
    later_keys = jnp.where(low & (lane > row), HIDDEN, 0.0)

    def gather_blocks():
        for count in range(1, n_kv):

            @pl.when(z == count)
            def _(count=count):
                kv_in(count).wait_recv()

        for source, start in ((kv_far, 0), (kv_own, n_kv * CAP)):
            both = source[...].astype(jnp.float32)
            left = lax.broadcasted_iota(jnp.int32, both.shape, 2) < HEAD_WIDTH
            keys[start : start + both.shape[0]] = jnp.where(left, both, 0.0).astype(jnp.bfloat16)
            values[start : start + both.shape[0]] = jnp.where(left, 1.0, both).astype(jnp.bfloat16)
        keys[absent] = jnp.where(lane == HEAD_WIDTH, HIDDEN, 0.0).astype(jnp.bfloat16)
        values[absent] = jnp.zeros((BLOCK_LENGTH, LANES), jnp.bfloat16)

    def chosen_rows(source, b):
        return jnp.concatenate([source[spots[b, s]] for s in range(picks)], axis=0)

    def score(part, b):
        query = query_rows[
            part * group : (part + 1) * group, b * BLOCK_LENGTH : (b + 1) * BLOCK_LENGTH, :
        ].reshape(group * BLOCK_LENGTH, LANES)
        return lax.dot_general(
            query, chosen_rows(keys, b), (((1,), (1,)), ((), ())),
            preferred_element_type=jnp.float32,
        )

    ahead = []

    def attend(part, start, count):
        for b in range(start, start + count):
            scores = ahead.pop() if ahead else score(part, b)
            if b + 1 < blocks:
                ahead.append(score(part, b + 1))
            scores = scores.reshape(group, BLOCK_LENGTH, picks * BLOCK_LENGTH)
            head, rest = scores[:, :, :LANES] + later_keys[None], scores[:, :, LANES:]
            top = jnp.maximum(
                jnp.max(head, axis=2, keepdims=True), jnp.max(rest, axis=2, keepdims=True)
            )
            expon = jnp.concatenate([jnp.exp(head - top), jnp.exp(rest - top)], axis=2)
            probs = expon.astype(jnp.bfloat16).reshape(group * BLOCK_LENGTH, picks * BLOCK_LENGTH)
            mixed = jnp.dot(probs, chosen_rows(values, b), preferred_element_type=jnp.float32)
            mixed = mixed.reshape(group, BLOCK_LENGTH, LANES)
            for p in range(group // 2):
                even, odd = mixed[2 * p], mixed[2 * p + 1]
                joined = jnp.where(
                    low,
                    pltpu.roll(even, HEAD_WIDTH, 1) / even,
                    odd / pltpu.roll(odd, HEAD_WIDTH, 1),
                )
                column = (part * group // 2 + p) * LANES
                attended[b * BLOCK_LENGTH : (b + 1) * BLOCK_LENGTH, column : column + LANES] = (
                    joined.astype(jnp.bfloat16)
                )

    loads[3].wait()
    for j in range(1, n_kv):
        ask(j).start()
    pltpu.make_async_copy(pair_own, pair_own, load_sem.at[5]).wait()
    out(1)
    query_loads[1].wait()
    for e in (6, 2, 0):
        out(e)
    query_loads[0].wait()
    for e in (4, 5):
        out(e)
    for e in (1, 6, 0):
        pass_on(e)
    out(3)
    loads[4].wait()
    plan_blocks()
    pass_on(2)
    out(7)
    pass_on(4)
    relay(0)
    pass_on(3)
    relay(1)
    loads[1].wait()
    for e in (10, 12, 8):
        out(e)
    relay(2)
    out(13)
    for e in (5, 7):
        pass_on(e)
    take(1)
    relay(3)
    take(0)
    relay(4)
    take(2)
    loads[0].wait()
    pair_stage()
    share_blocks()
    for e in (5, 6):
        relay(e)
    pass_on(8)
    out(9)
    pass_on(10)
    query_part(0, 0)
    take(3)
    relay(7)
    out(11)
    take(4)
    query_part(0, 1)
    take(5)
    query_part(0, 2)
    query_part(0, 3)
    out_far(12)
    out(14)
    query_tiles(0)
    out_far(13)
    gather_blocks()
    pass_on(9)
    attend(0, blocks * 0 // 2, blocks // 2)
    relay(8)
    pass_on(13)
    take(6)
    query_part(1, 0)
    query_part(1, 1)
    take(7)
    attend(0, blocks * 1 // 2, blocks // 2)
    pass_on(11)
    out_far(14)
    relay(10)
    query_part(1, 2)
    take(8)
    pass_on(12)
    query_part(1, 3)
    pass_on(14)
    query_tiles(1)
    relay(9)
    pass_far(13)
    attend(1, blocks * 0 // 2, blocks // 2)
    relay(11)
    attend(1, blocks * 1 // 2, blocks // 2)
    loads[2].wait()

    peer = lax.rem(t + 1, n_tp)
    other_rows = attended[pl.ds(pl.multiple_of(peer * half, half), half), :]
    own_rows = attended[pl.ds(pl.multiple_of(t * half, half), half), :]

    def swap_half(j):
        return remote(
            leaving.at[origin[j]], arriving.at[origin[j]], t_send.at[0], t_recv.at[j], "tp", peer
        )

    def project(j):
        weight = whole(2, j)
        leaving[origin[j]] = jnp.dot(
            other_rows, weight, preferred_element_type=jnp.float32
        ).astype(jnp.bfloat16)
        swap_half(j).start()
        kept[origin[j]] = jnp.dot(own_rows, weight, preferred_element_type=jnp.float32)

    relay(13)
    for e in (12, 14):
        pass_far(e)
    project(0)
    take(10)
    relay(12)
    take(9)
    project(1)
    relay(14)
    project(2)
    take(11)
    project(3)

    square = jnp.zeros((half, 1), jnp.float32)
    for j in range(n_kv):
        slot = origin[j]
        swap_half(j).wait_recv()
        mixed = kept[slot] + arriving[slot].astype(jnp.float32)
        kept[slot] = mixed
        square += jnp.sum(mixed * mixed, axis=1, keepdims=True)
    scale = lax.rsqrt(square * (1.0 / width) + 1e-06)
    for j in range(n_kv):
        columns = slice(j * depth, (j + 1) * depth)
        result[:, columns] = (kept[j] * scale * gain[:, columns]).astype(jnp.bfloat16)

    def drain(slots, sem):
        remote(slots, slots, sem, z_recv.at[0], "kv", origin[1]).wait_send()

    edge = out_all.shape[2] // PIECES[2] * (PIECES[2] - FAR)
    drain(pair_all.at[0 : n_kv - 1, 0:2], d_send.at[0])
    drain(query_all.at[0 : n_kv - 1, :, 0:2], d_send.at[1])
    drain(out_all.at[0 : n_kv - 1, 0:2], d_send.at[2])
    drain(pair_all.at[0 : n_kv - 1, 0], r_send.at[0])
    drain(query_all.at[0 : n_kv - 1, :, 0], r_send.at[1])
    if edge:
        drain(out_all.at[0 : n_kv - 1, 0, 0:edge], r_send.at[2])

    def drain_planes(planes):
        drain(pair_all.at[0:planes, 0], z_send.at[0])
        drain(query_all.at[0:planes, :, 0], z_send.at[1])
        drain(out_all.at[0:planes, 0], z_send.at[2])
        if FAR:
            drain(out_all.at[0:planes, 0, edge:], c_send.at[0])

    @pl.when(middle)
    def _():
        drain_planes(n_kv)

    @pl.when(jnp.logical_not(middle))
    def _():
        drain_planes(n_kv - 2)

    for count in range(1, n_kv):

        @pl.when(z == n_kv - 1 - count)
        def _(count=count):
            drain(packed.at[1 : count + 1], kv_send.at[0])

    drain(asks.at[0 : n_kv - 1], ask_send.at[0])
    drain(leaving, t_send.at[0])


def per_device_fused(
    n_dp, n_kv, n_tp,
    tokens, chosen, query_weight, key_matrix, value_matrix, out_weight, out_gain,
):
    rows, width = tokens.shape
    depth, columns = query_weight.shape
    blocks = rows // BLOCK_LENGTH
    cut = lambda w: w.reshape(n_dp, w.shape[0] // n_dp, w.shape[1])
    query, out = cut(query_weight), cut(out_weight)
    pair = jax.ShapeDtypeStruct((n_dp, LANES, depth // n_dp), jnp.bfloat16)
    bf16, f32 = jnp.bfloat16, jnp.float32
    vmem = pl.BlockSpec(memory_space=pltpu.VMEM)
    off_core = pl.BlockSpec(memory_space=pltpu.HBM)
    dma = pltpu.SemaphoreType.DMA
    copies = sum(PIECES) * (n_kv - 1)
    return pl.pallas_call(
        functools.partial(fused, n_dp, n_kv, n_tp),
        out_shape=pltpu.VMEM((rows // n_tp, width), bf16),
        in_specs=[
            off_core, off_core, off_core, off_core, off_core, off_core, off_core,
        ],
        out_specs=vmem,
        scratch_shapes=[
            pltpu.SMEM((blocks, chosen.shape[1]), jnp.int32),
            pltpu.SMEM((blocks, chosen.shape[1]), jnp.int32),
            pltpu.SMEM((n_kv,), jnp.int32),
            pltpu.SMEM((n_kv, 2), jnp.int32),
            pltpu.VMEM((1, width), f32),
            pltpu.VMEM((rows, width), bf16),
            pltpu.VMEM(pair.shape, bf16),
            pltpu.VMEM((PIECES[1],) + query.shape[:2] + (columns // PIECES[1],), bf16),
            pltpu.VMEM(out.shape, bf16),
            pltpu.VMEM((blocks, chosen.shape[1]), jnp.int32),
            pltpu.VMEM((n_kv, blocks, chosen.shape[1]), jnp.int32),
            pltpu.VMEM((n_kv, CAP, BLOCK_LENGTH, LANES), bf16),
            pltpu.VMEM((blocks, BLOCK_LENGTH, LANES), bf16),
            pltpu.VMEM((n_kv * CAP, BLOCK_LENGTH, LANES), bf16),
            pltpu.VMEM((n_kv,) + pair.shape, bf16),
            pltpu.VMEM(
                (n_kv, PIECES[1]) + query.shape[:2] + (columns // PIECES[1],), bf16
            ),
            pltpu.VMEM((n_kv,) + out.shape, bf16),
            pltpu.VMEM((n_kv * CAP + blocks + 1, BLOCK_LENGTH, LANES), bf16),
            pltpu.VMEM((n_kv * CAP + blocks + 1, BLOCK_LENGTH, LANES), bf16),
            pltpu.VMEM((rows, columns // PIECES[1]), f32),
            pltpu.VMEM((columns // HEAD_WIDTH, rows, LANES), bf16),
            pltpu.VMEM((rows, columns), bf16),
            pltpu.VMEM((n_kv, rows // n_tp, width // n_kv), bf16),
            pltpu.VMEM((n_kv, rows // n_tp, width // n_kv), bf16),
            pltpu.VMEM((n_kv, rows // n_tp, width // n_kv), f32),
            dma((6 + PIECES[1],)), dma((3,)), dma((copies,)), dma((1,)), dma((max(1, FAR * (n_kv - 1)),)),
            dma((3,)), dma((copies,)), dma((3,)), dma((copies,)),
            dma((1,)), dma((1,)), dma((1,)), dma((n_kv,)), dma((1,)), dma((1,)),
        ],
        compiler_params=pltpu.CompilerParams(
            collective_id=0, has_side_effects=True, vmem_limit_bytes=54 * 1024 * 1024
        ),
    )(chosen, tokens, key_matrix.T, value_matrix.T, query, out, out_gain.reshape(1, width))


def per_device(tokens, chosen, query_weight, key_matrix, value_matrix, out_weight, out_gain):
    tok_rows = tokens.shape[0]
    blocks = tok_rows // BLOCK_LENGTH
    device = lax.axis_index("kv")
    kv_count = lax.axis_size("kv")
    whole_query, whole_key, whole_value = (
        lax.all_gather(query_weight, "kv", axis=0, tiled=True),
        lax.all_gather(key_matrix, "kv", axis=0, tiled=True),
        lax.all_gather(value_matrix, "kv", axis=0, tiled=True),
    )
    query_rows = jnp.dot(tokens, whole_query, preferred_element_type=jnp.float32).astype(
        jnp.bfloat16
    )
    key_rows = jnp.dot(tokens, whole_key, preferred_element_type=jnp.float32).astype(jnp.bfloat16)
    value_rows = jnp.dot(tokens, whole_value, preferred_element_type=jnp.float32).astype(
        jnp.bfloat16
    )
    paired = jnp.concatenate([key_rows, value_rows], axis=1)
    pair_width = paired.shape[1]
    safe_ids = jnp.maximum(chosen, 0)
    everyone = lax.all_gather(paired, "kv", axis=0, tiled=True).reshape(
        kv_count * blocks, BLOCK_LENGTH, pair_width
    )
    picked = jnp.take(everyone, safe_ids, axis=0)
    head_count = query_rows.shape[1] // HEAD_WIDTH
    grouped = query_rows.reshape(blocks, BLOCK_LENGTH, head_count, HEAD_WIDTH)
    offsets = jnp.arange(BLOCK_LENGTH, dtype=jnp.int32)
    query_pos = (device * blocks + jnp.arange(blocks, dtype=jnp.int32))[
        :, None
    ] * BLOCK_LENGTH + offsets[None, :]
    key_pos = safe_ids[:, :, None] * BLOCK_LENGTH + offsets[None, None, :]
    visible = (chosen >= 0)[:, None, :, None] & (
        key_pos[:, None, :, :] <= query_pos[:, :, None, None]
    )

    def attend_block(inputs):
        query_block, pair_block, seen = inputs
        block_keys = pair_block[..., :HEAD_WIDTH]
        block_values = pair_block[..., HEAD_WIDTH:]
        scores = jnp.einsum(
            "qgd,skd->gqsk", query_block, block_keys, preferred_element_type=jnp.float32
        ) * HEAD_WIDTH ** (-0.5)
        scores = jnp.where(seen[None], scores, -1e30)
        row_max = jnp.max(scores, axis=(2, 3), keepdims=True)
        expon = jnp.exp(scores - row_max)
        row_sum = jnp.sum(expon, axis=(2, 3), keepdims=True)
        weights_bf = (expon / row_sum).astype(jnp.bfloat16)
        result = jnp.einsum(
            "gqsk,skd->qgd", weights_bf, block_values, preferred_element_type=jnp.float32
        )
        return result.astype(jnp.bfloat16)

    attended = lax.map(attend_block, (grouped, picked, visible))
    attended = attended.reshape(tok_rows, head_count * HEAD_WIDTH)
    whole_out = lax.all_gather(out_weight, "kv", axis=1, tiled=True)
    mixed = lax.psum_scatter(
        jnp.dot(attended, whole_out, preferred_element_type=jnp.float32).astype(jnp.bfloat16),
        "tp",
        scatter_dimension=0,
        tiled=True,
    ).astype(jnp.float32)
    normed = mixed * lax.rsqrt(jnp.mean(mixed * mixed, axis=-1, keepdims=True) + 1e-06) * out_gain
    return normed.astype(jnp.bfloat16)


def solution(mesh):
    placed = (
        P(("dp", "kv"), None),
        P(("dp", "kv"), None),
        P("kv", "tp"),
        P("kv", "tp"),
        P("kv", "tp"),
        P("tp", "kv"),
        P(),
    )
    n_dp, n_kv, n_tp = (mesh.shape[name] for name in ("dp", "kv", "tp"))

    def body(tokens, chosen, query_weight, key_matrix, value_matrix, out_weight, out_gain):
        args = (tokens, chosen, query_weight, key_matrix, value_matrix, out_weight, out_gain)
        depth, columns = query_weight.shape
        whole_tiles = (
            depth % (LANES * n_dp) == 0
            and columns % (2 * LANES * PIECES[1]) == 0
            and columns % (2 * LANES * PIECES[1]) == 0
            and out_weight.shape[0] % (32 * PIECES[2] * n_dp) == 0
            and out_weight.shape[1] % LANES == 0
            and columns % LANES == 0
            and key_matrix.shape[1] == HEAD_WIDTH
            and chosen.shape[1] % 2 == 0
            and n_tp == 2
            and n_dp == 4
            and n_kv == 4
            and tokens.shape[0] == 8 * BLOCK_LENGTH
        )
        if whole_tiles:
            return per_device_fused(n_dp, n_kv, n_tp, *args)
        return per_device(*args)

    return jax.shard_map(
        body,
        mesh=mesh,
        in_specs=placed,
        out_specs=P(("dp", "kv", "tp"), None),
        check_vma=False,
    )
```
